128 devices in a mesh: fs: 16 (over z, x), tp: 8 (over y, core).
Axes of the slice: x: 4, y: 4, z: 4, core: 2. Of those that a mesh axis runs over, the one named last changes fastest.
Arguments:
- layer_inputs: bfloat16 [40960, 2048], P('fs'), may hold values from -6 to 6
- output_cot: bfloat16 [40960, 2048], P('fs'), may hold values from -6 to 6
- query_cot: bfloat16 [40960, 2048], P('fs', 'tp'), may hold values from -6 to 6
- head_outputs: bfloat16 [40960, 2048], P('fs', 'tp'), may hold values from -6 to 6
- weights: float32 [2, 2048, 2048], P(None, 'fs', 'tp'), may hold values from -0.125 to 0.125
- factors: bfloat16 [2, 2048, 256], replicated, may hold values from -0.125 to 0.125
- first_moment: float32 [2, 256, 2048], P(None, None, 'tp'), may hold values from -600 to 600
- second_moment: float32 [2, 256, 2048], P(None, None, 'tp'), may hold values from 1000 to 100000
Outputs:
- new_weights: float32 [2, 2048, 2048], P(None, 'fs', 'tp')
- update: float32 [2, 2048, 2048], P(None, 'fs', 'tp')
- new_first: float32 [2, 256, 2048], P(None, None, 'tp')
- new_second: float32 [2, 256, 2048], P(None, None, 'tp')
- weight_copy: bfloat16 [2, 2048, 2048], P(None, None, 'tp')
The draws below stay inside these ranges and needn't reach their ends.
All inputs are finite; a program needn't handle non-finite values.
Results may differ from the reference program's by a relative error of at most 0.00055.
Values may be sent and summed in bfloat16 or wider, within the bound.
A program may use at most 128 MiB of HBM per device.

```python
import math
import jax
import jax.numpy as jnp
from jax import lax

D = 2048
QDIM = 2048
RANK = 256
TOKENS = 40960


def block_scale(own_key, shape, split, smallest, high):
    def one(dim, blocks):
        steps = jax.random.uniform(jax.random.fold_in(jax.random.fold_in(own_key, 6), dim), (blocks,), jnp.float32, smallest / len(split), high / len(split))
        return jnp.repeat(jnp.exp(steps), shape[dim] // blocks).reshape((-1,) + (1,) * (len(shape) - dim - 1))

    loudness = one(*split[0])
    for cut in split[1:]:
        loudness = loudness * one(*cut)
    return loudness


def noise(own_key, extent, spread, reach, cuts=(), kind=jnp.bfloat16):
    result = spread * jax.random.normal(own_key, extent, jnp.float32)
    if cuts:
        result = result * block_scale(own_key, extent, cuts, -0.22, 0.18)
    return jnp.clip(result, -reach, reach).astype(kind)


def setup_inputs(seed: int = 0) -> dict:
    streams_of = jax.random.split(jax.random.key(seed), 9)
    return {
        "layer_inputs": noise(streams_of[0], (TOKENS, D), 1.0, 6.0, ((0, 16),)),
        "output_cot": noise(streams_of[1], (TOKENS, D), 1.0, 6.0, ((0, 16),)),
        "query_cot": noise(streams_of[2], (TOKENS, QDIM), 1.0, 6.0, ((0, 16), (1, 8))),
        "head_outputs": noise(streams_of[3], (TOKENS, QDIM), 1.0, 6.0, ((0, 16), (1, 8))),
        "weights": noise(streams_of[4], (2, D, QDIM), D ** -0.5, 0.125, ((1, 16), (2, 8)), jnp.float32),
        "factors": noise(streams_of[5], (2, D, RANK), D ** -0.5, 0.125),
        "first_moment": noise(streams_of[6], (2, RANK, QDIM), 100.0, 600.0, ((2, 8),), jnp.float32),
        "second_moment": jnp.clip(jnp.exp(math.log(100000.0) - 4.6051702 * jax.random.uniform(streams_of[7], (2, RANK, QDIM), jnp.float32) ** block_scale(streams_of[7], (2, RANK, QDIM), ((2, 8),), -0.2, 0.2)), 1000.0, 100000.0),
    }


def reference(layer_inputs, output_cot, query_cot, head_outputs, weights, factors, first_moment, second_moment):
    lefts = (layer_inputs, output_cot)
    rights = (query_cot, head_outputs)
    steps = []
    firsts = []
    seconds = []
    for index in range(2):
        grad = jnp.dot(lefts[index].T, rights[index], preferred_element_type=jnp.float32)
        factor = factors[index].astype(jnp.float32)
        low = jnp.dot(factor.T, grad, precision=lax.Precision.HIGHEST)
        first = 0.9 * first_moment[index] + 0.1 * low
        second = 0.95 * second_moment[index] + 0.05 * low * low
        normed = first / (jnp.sqrt(second) + 1e-06)
        ratio = jnp.sqrt(jnp.sum(normed * normed)) / jnp.sqrt(jnp.sum(low * low) + 1e-06)
        resid = grad - jnp.dot(factor, low, precision=lax.Precision.HIGHEST)
        steps.append(jnp.dot(factor, normed, precision=lax.Precision.HIGHEST) + ratio * resid)
        firsts.append(first)
        seconds.append(second)
    step = jnp.stack(steps)
    update = step * lax.rsqrt(jnp.mean(step * step) + 1e-06)
    new_weights = weights - 0.02 * update
    return (new_weights, update, jnp.stack(firsts), jnp.stack(seconds), new_weights.astype(jnp.bfloat16))
```

```python
import jax
import jax.numpy as jnp
from jax import lax
from jax.experimental import pallas as pl
from jax.experimental.pallas import tpu as pltpu
from jax.sharding import Mesh
from jax.sharding import PartitionSpec as P

Z, X, Y, C = "fs_0", "fs_1", "tp_0", "tp_1"
FS, TP = (Z, X), (Y, C)
MESH = pl.DeviceIdType.MESH
F32, BF16 = jnp.float32, jnp.bfloat16
ORDER = (2, 1, 3, 0)


class Copies:
    def __init__(self, send_sems, recv_sems):
        self.send_sems, self.recv_sems, self.made = send_sems, recv_sems, []

    def send(self, src, dst, device):
        index = len(self.made)
        copy = pltpu.make_async_remote_copy(
            src_ref=src,
            dst_ref=dst,
            send_sem=self.send_sems.at[index],
            recv_sem=self.recv_sems.at[index],
            device_id=device,
            device_id_type=MESH,
        )
        copy.start()
        self.made.append(copy)
        return copy


COPIES = 160
LOADS = 24


def halves(value, terms):
    out = []
    for _ in range(terms - 1):
        part = value.astype(BF16)
        out.append(part)
        value = value - part.astype(F32)
    out.append(value.astype(BF16))
    return out


def folded(value):
    rows, cols = value.shape
    total = value[:, 0:128]
    for start in range(128, cols, 128):
        total = total + value[:, start : start + 128]
    return total.reshape(rows // 8, 8, 128).sum(axis=0)


def kernel(
    layer_inputs, output_cot, query_cot, head_outputs, weights, factors, first_moment, second_moment,
    new_weights, update, new_first, new_second, weight_copy,
    left, right, right_t, fact, grad, one_a, one_b, two_a, two_b,
    low_t, low_in1, low_in2, low_all, wts, mom1, mom2, out_w, out_u, gathered,
    own_p, own_f, tp_own, tp_in, fs_own, fs_in, tot_own, tot_in,
    load_sems, store_sems, send_sems, recv_sems,
):
    z, x, y, c = (lax.axis_index(name) for name in (Z, X, Y, C))
    lefts, rights = (layer_inputs, output_cot), (query_cot, head_outputs)
    coord = {Z: z, X: x, Y: y, C: c}
    axes = ((X, Z), (Z, X))

    def near(axis, delta):
        return {axis: lax.rem(coord[axis] + delta, 4)}

    def place(k, a, b):
        first, second = axes[k]
        at = {first: lax.rem(coord[first] + b, 4), second: lax.rem(coord[second] + a, 4)}
        return at[Z] * 4 + at[X]

    loads = []

    def load(pairs, whole):
        sem = load_sems.at[len(loads)]
        for src, dst in pairs:
            pltpu.make_async_copy(src, dst, sem).start()
        loads.append(pltpu.make_async_copy(whole, whole, sem))
        return loads[-1]

    def load_left(k, a):
        pairs = []
        for b in range(4):
            cols = pl.ds(pl.multiple_of(place(k, a, b) * 128, 128), 128)
            pairs.append((lefts[k].at[:, cols], left.at[k, a, :, pl.ds(128 * b, 128)]))
        return load(pairs, left.at[k, a])

    def load_factors(k):
        pairs = []
        for a in range(4):
            for b in range(4):
                rows = pl.ds(pl.multiple_of(place(k, a, b) * 128, 128), 128)
                pairs.append((factors.at[k, rows, :], fact.at[k, a, pl.ds(128 * b, 128), :]))
        return load(pairs, fact.at[k])

    right_in, left_in, fact_in = [None] * 2, {}, [None] * 2
    for k in range(2):
        right_in[k] = load([(rights[k], right.at[k])], right.at[k])
        left_in[k, ORDER[0]] = load_left(k, ORDER[0])
    for k in range(2):
        left_in[k, ORDER[1]] = load_left(k, ORDER[1])
    for k in range(2):
        fact_in[k] = load_factors(k)
    for a in ORDER[2:]:
        for k in range(2):
            left_in[k, a] = load_left(k, a)
    mom1_in = load([(first_moment, mom1)], mom1)
    mom2_in = load([(second_moment, mom2)], mom2)
    wts_in = load([(weights, wts)], wts)

    barrier = pltpu.get_barrier_semaphore()
    fs_peers = [
        {Z: lax.rem(z + dz, 4), X: lax.rem(x + dx, 4)} for dz in range(4) for dx in range(4) if dz or dx
    ]
    tp_peers = [
        {Y: lax.rem(y + dy, 4), C: lax.rem(c + dc, 2)} for dy in range(4) for dc in range(2) if dy or dc
    ]
    for peer in fs_peers + tp_peers:
        pl.semaphore_signal(barrier, inc=1, device_id=peer, device_id_type=MESH)

    copies = Copies(send_sems, recv_sems)
    top, bottom = pl.ds(0, 128), pl.ds(128, 128)

    def transpose_right(k):
        right_in[k].wait()
        for start in range(0, 2560, 256):
            right_t[k, :, start : start + 256] = right[k, start : start + 256, :].T

    def local_grad(k, a):
        left_in[k, a].wait()
        value = jnp.dot(right_t[k], left[k, a], preferred_element_type=F32)
        for b in range(4):
            grad[k, a, b] = value[:, 128 * b : 128 * b + 128]

    def local_low(k, a):
        total = None
        for b in range(4):
            block = grad[k, a, b]
            rows = fact[k, a, 128 * b : 128 * b + 128, :]
            for part in halves(block, 2):
                term = jnp.dot(part, rows, preferred_element_type=F32)
                total = term if total is None else total + term
        if a == ORDER[0]:
            low_t[k] = total
        else:
            low_t[k] = low_t[k] + total

    pending = {}

    def one_start(k, a):
        axis = axes[k][0]
        got = {}
        got["a0"] = copies.send(grad.at[k, a, 2, top], one_a.at[k, a, 0], near(axis, 1))
        got["a1"] = copies.send(grad.at[k, a, 2, bottom], one_a.at[k, a, 1], near(axis, 3))
        got["b01"] = copies.send(grad.at[k, a, 1, bottom], one_b.at[k, a, 0, 1], near(axis, 1))
        got["b10"] = copies.send(grad.at[k, a, 3, top], one_b.at[k, a, 1, 0], near(axis, 3))
        pending["one", k, a] = got

    def one_forward(k, a):
        axis = axes[k][0]
        got = pending["one", k, a]
        got["a0"].wait_recv()
        grad[k, a, 1, 0:128] = grad[k, a, 1, 0:128] + one_a[k, a, 0]
        got["b00"] = copies.send(grad.at[k, a, 1, top], one_b.at[k, a, 0, 0], near(axis, 1))
        got["a1"].wait_recv()
        grad[k, a, 3, 128:256] = grad[k, a, 3, 128:256] + one_a[k, a, 1]
        got["b11"] = copies.send(grad.at[k, a, 3, bottom], one_b.at[k, a, 1, 1], near(axis, 3))

    def one_finish(k, a):
        got = pending["one", k, a]
        got["b01"].wait_recv()
        got["b10"].wait_recv()
        got["b00"].wait_recv()
        grad[k, a, 0, 0:128] = grad[k, a, 0, 0:128] + (one_b[k, a, 0, 0] + one_b[k, a, 1, 0])
        got["b11"].wait_recv()
        grad[k, a, 0, 128:256] = grad[k, a, 0, 128:256] + (one_b[k, a, 0, 1] + one_b[k, a, 1, 1])

    def two_start(k):
        axis = axes[k][1]
        got = pending["two", k] = {}
        got["a0"] = copies.send(grad.at[k, 2, 0, top], two_a.at[k, 0], near(axis, 1))
        got["a1"] = copies.send(grad.at[k, 2, 0, bottom], two_a.at[k, 1], near(axis, 3))

    def two_plus(k):
        axis = axes[k][1]
        got = pending["two", k]
        got["b01"] = copies.send(grad.at[k, 1, 0, bottom], two_b.at[k, 0, 1], near(axis, 1))
        got["a0"].wait_recv()
        grad[k, 1, 0, 0:128] = grad[k, 1, 0, 0:128] + two_a[k, 0]
        got["b00"] = copies.send(grad.at[k, 1, 0, top], two_b.at[k, 0, 0], near(axis, 1))

    def two_minus(k):
        axis = axes[k][1]
        got = pending["two", k]
        got["b10"] = copies.send(grad.at[k, 3, 0, top], two_b.at[k, 1, 0], near(axis, 3))
        got["a1"].wait_recv()
        grad[k, 3, 0, 128:256] = grad[k, 3, 0, 128:256] + two_a[k, 1]
        got["b11"] = copies.send(grad.at[k, 3, 0, bottom], two_b.at[k, 1, 1], near(axis, 3))

    def two_finish(k):
        got = pending["two", k]
        for name in ("b01", "b10", "b00", "b11"):
            got[name].wait_recv()
        top_sum = grad[k, 0, 0, 0:128] + (two_b[k, 0, 0] + two_b[k, 1, 0])
        bottom_sum = grad[k, 0, 0, 128:256] + (two_b[k, 0, 1] + two_b[k, 1, 1])
        return jnp.concatenate([top_sum, bottom_sum], axis=0)

    def low_rows(k, b, a=None):
        first, second = axes[k]
        start = lax.rem(coord[first] + b, 4) * 64
        if a is None:
            return pl.ds(pl.multiple_of(start, 64), 64)
        return pl.ds(pl.multiple_of(start + lax.rem(coord[second] + a, 4) * 16, 16), 16)

    def low_one(k):
        pending["l1", k] = [
            copies.send(low_t.at[k, low_rows(k, b)], low_in1.at[k, 3 - b], near(axes[k][0], b)) for b in (2, 1, 3)
        ]

    def low_two(k):
        for copy in pending["l1", k]:
            copy.wait_recv()
        rows = low_rows(k, 0)
        low_t[k, rows] = low_t[k, rows] + low_in1[k, 0] + low_in1[k, 1] + low_in1[k, 2]
        pending["l2", k] = [
            copies.send(low_t.at[k, low_rows(k, 0, a)], low_in2.at[k, 3 - a], near(axes[k][1], a)) for a in (2, 1, 3)
        ]

    def low_three(k):
        for copy in pending["l2", k]:
            copy.wait_recv()
        rows = low_rows(k, 0, 0)
        low_all[k, rows] = low_t[k, rows] + low_in2[k, 0] + low_in2[k, 1] + low_in2[k, 2]
        pending["l3", k] = [
            copies.send(low_all.at[k, rows], low_all.at[k, rows], near(axes[k][1], a)) for a in (2, 1, 3)
        ]

    def low_four(k):
        for copy in pending["l3", k]:
            copy.wait_recv()
        rows = low_rows(k, 0)
        pending["l4", k] = [
            copies.send(low_all.at[k, rows], low_all.at[k, rows], near(axes[k][0], b)) for b in (2, 1, 3)
        ]

    stores = []

    def store(src, dst):
        copy = pltpu.make_async_copy(src, dst, store_sems.at[len(stores)])
        copy.start()
        stores.append(copy)

    def moments(k):
        for copy in pending["l4", k]:
            copy.wait_recv()
        low = low_all[k].T
        first = 0.9 * mom1[k] + 0.1 * low
        second = 0.95 * mom2[k] + 0.05 * low * low
        mom1[k] = first
        mom2[k] = second
        normed = first / (jnp.sqrt(second) + 1e-06)
        tp_own[k] = folded(normed * normed)
        tp_own[2 + k] = folded(low * low)
        mine = fact[k, 0, 0:128, :]
        own_p[k] = sum(jnp.dot(mine, part, preferred_element_type=F32) for part in halves(normed, 3))
        own_f[k] = sum(jnp.dot(mine, part, preferred_element_type=F32) for part in halves(low, 3))

    last = None
    for step, a in enumerate(ORDER):
        for k in range(2):
            if step == 0:
                transpose_right(k)
            local_grad(k, a)
            if step == 0 and k == 0:
                pl.semaphore_wait(barrier, len(fs_peers) + len(tp_peers))
            if step < 2:
                one_start(k, a)
            if step == 1:
                one_forward(k, ORDER[0])
        for k in range(2):
            if step == 0:
                fact_in[k].wait()
            local_low(k, a)
    for k in range(2):
        low_one(k)
    for k in range(2):
        one_forward(k, ORDER[1])
        one_start(k, ORDER[2])
        one_finish(k, ORDER[0])
        two_start(k)
    for k in range(2):
        low_two(k)
    for k in range(2):
        one_forward(k, ORDER[2])
        one_start(k, ORDER[3])
        one_finish(k, ORDER[1])
        two_plus(k)
    for k in range(2):
        low_three(k)
    for k in range(2):
        one_forward(k, ORDER[3])
        one_finish(k, ORDER[2])
        two_minus(k)
    for k in range(2):
        low_four(k)
    mom1_in.wait()
    mom2_in.wait()
    for k in range(2):
        moments(k)
    store(mom1, new_first)
    store(mom2, new_second)
    tp_copies = [copies.send(tp_own, tp_in.at[i], peer) for i, peer in enumerate(tp_peers)]
    for k in range(2):
        one_finish(k, ORDER[3])
    for copy in tp_copies:
        copy.wait_recv()
    sums = tp_own[...]
    for i in range(len(tp_peers)):
        sums = sums + tp_in[i]
    wts_in.wait()

    square = None
    for k in range(2):
        normed_sum = jnp.sum(sums[k], keepdims=True)
        low_sum = jnp.sum(sums[2 + k], keepdims=True)
        ratio = jnp.sqrt(normed_sum) / jnp.sqrt(low_sum + 1e-06)
        own = two_finish(k).T
        step = own_p[k] + ratio * (own - own_f[k])
        out_u[k] = step
        term = folded(step * step)
        square = term if square is None else square + term
    tot_own[...] = square
    tot_copies = [copies.send(tot_own, tot_in.at[i], peer) for i, peer in enumerate(tp_peers)]
    for copy in tot_copies:
        copy.wait_recv()
    for i in range(len(tp_peers)):
        square = square + tot_in[i]
    fs_own[...] = square
    fs_copies = [copies.send(fs_own, fs_in.at[i], peer) for i, peer in enumerate(fs_peers)]
    for copy in fs_copies:
        copy.wait_recv()
    for i in range(len(fs_peers)):
        square = square + fs_in[i]
    total = jnp.sum(square, keepdims=True)
    scale = lax.rsqrt(total / (2.0 * 2048 * 2048) + 1e-06)

    for k in range(2):
        value = out_u[k] * scale
        out_u[k] = value
        value = wts[k] - 0.02 * value
        out_w[k] = value
        gathered[k, 0, 0] = value.astype(BF16)
    store(out_u, update)
    store(out_w, new_weights)

    def put(k, a, b):
        rows = pl.ds(pl.multiple_of(place(k, a, b) * 128, 128), 128)
        store(gathered.at[k, a, b], weight_copy.at[k, rows, :])

    upper, lower = pl.ds(0, 64), pl.ds(64, 64)

    def spread(k, b):
        block = gathered.at[k, 0, b]
        got = pending["w", k, b] = {}
        got["plus"] = copies.send(block, gathered.at[k, 3, b], near(axes[k][1], 1))
        got["minus"] = copies.send(block, gathered.at[k, 1, b], near(axes[k][1], 3))
        put(k, 0, b)

    def relay(k, b):
        got = pending["w", k, b]
        got["plus"].wait_recv()
        got["far0"] = copies.send(gathered.at[k, 3, b, upper], gathered.at[k, 2, b, upper], near(axes[k][1], 1))
        put(k, 3, b)
        got["minus"].wait_recv()
        got["far1"] = copies.send(gathered.at[k, 1, b, lower], gathered.at[k, 2, b, lower], near(axes[k][1], 3))
        put(k, 1, b)

    def land(k, b):
        got = pending["w", k, b]
        got["far0"].wait_recv()
        got["far1"].wait_recv()
        put(k, 2, b)

    for k in range(2):
        axis = axes[k][0]
        got = pending["v", k] = {}
        got["plus"] = copies.send(gathered.at[k, 0, 0], gathered.at[k, 0, 3], near(axis, 1))
        got["minus"] = copies.send(gathered.at[k, 0, 0], gathered.at[k, 0, 1], near(axis, 3))
    for k in range(2):
        spread(k, 0)
    for k in range(2):
        axis = axes[k][0]
        got = pending["v", k]
        got["plus"].wait_recv()
        got["far0"] = copies.send(gathered.at[k, 0, 3, upper], gathered.at[k, 0, 2, upper], near(axis, 1))
        got["minus"].wait_recv()
        got["far1"] = copies.send(gathered.at[k, 0, 1, lower], gathered.at[k, 0, 2, lower], near(axis, 3))
        spread(k, 3)
        spread(k, 1)
    for k in range(2):
        relay(k, 0)
    for k in range(2):
        got = pending["v", k]
        got["far0"].wait_recv()
        got["far1"].wait_recv()
        spread(k, 2)
    for b in (3, 1, 2):
        for k in range(2):
            relay(k, b)
    for b in (0, 3, 1, 2):
        for k in range(2):
            land(k, b)
    for copy in copies.made:
        copy.wait_send()
    for copy in stores:
        copy.wait()


def per_device(*args):
    any_space = pl.BlockSpec(memory_space=pl.ANY)
    shapes = (
        ((2, 128, 256), F32),
        ((2, 128, 256), F32),
        ((2, 256, 256), F32),
        ((2, 256, 256), F32),
        ((2, 2048, 256), BF16),
    )
    dma = pltpu.SemaphoreType.DMA
    return pl.pallas_call(
        kernel,
        name="step",
        out_shape=[jax.ShapeDtypeStruct(*shape) for shape in shapes],
        in_specs=[any_space] * 8,
        out_specs=[any_space] * 5,
        scratch_shapes=[
            pltpu.VMEM((2, 4, 2560, 512), BF16),
            pltpu.VMEM((2, 2560, 256), BF16),
            pltpu.VMEM((2, 256, 2560), BF16),
            pltpu.VMEM((2, 4, 512, 256), BF16),
            pltpu.VMEM((2, 4, 4, 256, 128), F32),
            pltpu.VMEM((2, 4, 2, 128, 128), F32),
            pltpu.VMEM((2, 4, 2, 2, 128, 128), F32),
            pltpu.VMEM((2, 2, 128, 128), F32),
            pltpu.VMEM((2, 2, 2, 128, 128), F32),
            pltpu.VMEM((2, 256, 256), F32),
            pltpu.VMEM((2, 3, 64, 256), F32),
            pltpu.VMEM((2, 3, 16, 256), F32),
            pltpu.VMEM((2, 256, 256), F32),
            pltpu.VMEM((2, 128, 256), F32),
            pltpu.VMEM((2, 256, 256), F32),
            pltpu.VMEM((2, 256, 256), F32),
            pltpu.VMEM((2, 128, 256), F32),
            pltpu.VMEM((2, 128, 256), F32),
            pltpu.VMEM((2, 4, 4, 128, 256), BF16),
            pltpu.VMEM((2, 128, 256), F32),
            pltpu.VMEM((2, 128, 256), F32),
            pltpu.VMEM((4, 8, 128), F32),
            pltpu.VMEM((7, 4, 8, 128), F32),
            pltpu.VMEM((8, 128), F32),
            pltpu.VMEM((15, 8, 128), F32),
            pltpu.VMEM((8, 128), F32),
            pltpu.VMEM((7, 8, 128), F32),
            dma((LOADS,)),
            dma((40,)),
            dma((COPIES,)),
            dma((COPIES,)),
        ],
        compiler_params=pltpu.CompilerParams(
            collective_id=0, has_side_effects=True, vmem_limit_bytes=60 * 1024 * 1024
        ),
    )(*args)


def solution(mesh):
    finer = Mesh(mesh.devices.reshape(4, 4, 4, 2), (Z, X, Y, C))
    in_specs = (
        P(FS, None),
        P(FS, None),
        P(FS, TP),
        P(FS, TP),
        P(None, FS, TP),
        P(),
        P(None, None, TP),
        P(None, None, TP),
    )
    out_specs = (
        P(None, FS, TP),
        P(None, FS, TP),
        P(None, None, TP),
        P(None, None, TP),
        P(None, None, TP),
    )
    return jax.shard_map(per_device, mesh=finer, in_specs=in_specs, out_specs=out_specs, check_vma=False)
```

```python
import jax
import jax.numpy as jnp
from jax import lax
from jax.experimental import pallas as pl
from jax.experimental.pallas import tpu as pltpu
from jax.sharding import Mesh
from jax.sharding import PartitionSpec as P

Z, X, Y, C = "fs_0", "fs_1", "tp_0", "tp_1"
FS, TP = (Z, X), (Y, C)
MESH = pl.DeviceIdType.MESH
F32, BF16 = jnp.float32, jnp.bfloat16
ORDER = (2, 1, 3, 0)


class Copies:
    def __init__(self, send_sems, recv_sems):
        self.send_sems, self.recv_sems, self.made = send_sems, recv_sems, []

    def send(self, src, dst, device):
        index = len(self.made)
        copy = pltpu.make_async_remote_copy(
            src_ref=src,
            dst_ref=dst,
            send_sem=self.send_sems.at[index],
            recv_sem=self.recv_sems.at[index],
            device_id=device,
            device_id_type=MESH,
        )
        copy.start()
        self.made.append(copy)
        return copy


COPIES = 192
LOADS = 24


def halves(value, terms):
    out = []
    for _ in range(terms - 1):
        part = value.astype(BF16)
        out.append(part)
        value = value - part.astype(F32)
    out.append(value.astype(BF16))
    return out


def folded(value):
    rows, cols = value.shape
    total = value[:, 0:128]
    for start in range(128, cols, 128):
        total = total + value[:, start : start + 128]
    return total.reshape(rows // 8, 8, 128).sum(axis=0)


def kernel(
    layer_inputs, output_cot, query_cot, head_outputs, weights, factors, first_moment, second_moment,
    out_w, out_u, out_1, out_2, gathered,
    left, right, right_t, fact, grad, one_a, one_b, two_a, two_b,
    low_t, low_a, low_b, low_in, low_all, wts, mom1, mom2,
    own_p, own_f, tp_own, tp_in, tot_own, tot_in, last_own, last_in,
    load_sems, send_sems, recv_sems,
):
    z, x, y, c = (lax.axis_index(name) for name in (Z, X, Y, C))
    lefts, rights = (layer_inputs, output_cot), (query_cot, head_outputs)
    coord = {Z: z, X: x, Y: y, C: c}
    axes = ((X, Z), (Z, X))

    def near(axis, delta):
        return {axis: lax.rem(coord[axis] + delta, 4)}

    def place(k, a, b):
        first, second = axes[k]
        at = {first: lax.rem(coord[first] + b, 4), second: lax.rem(coord[second] + a, 4)}
        return at[Z] * 4 + at[X]

    loads = []

    def load(pairs, whole):
        sem = load_sems.at[len(loads)]
        for src, dst in pairs:
            pltpu.make_async_copy(src, dst, sem).start()
        loads.append(pltpu.make_async_copy(whole, whole, sem))
        return loads[-1]

    def load_left(k, a):
        pairs = []
        for b in range(4):
            cols = pl.ds(pl.multiple_of(place(k, a, b) * 128, 128), 128)
            pairs.append((lefts[k].at[:, cols], left.at[k, a, :, pl.ds(128 * b, 128)]))
        return load(pairs, left.at[k, a])

    def load_factors(k):
        pairs = []
        for a in range(4):
            for b in range(4):
                rows = pl.ds(pl.multiple_of(place(k, a, b) * 128, 128), 128)
                pairs.append((factors.at[k, rows, :], fact.at[k, a, pl.ds(128 * b, 128), :]))
        return load(pairs, fact.at[k])

    right_in, left_in, fact_in = [None] * 2, {}, [None] * 2
    for k in range(2):
        right_in[k] = load([(rights[k], right.at[k])], right.at[k])
        left_in[k, ORDER[0]] = load_left(k, ORDER[0])
    for k in range(2):
        left_in[k, ORDER[1]] = load_left(k, ORDER[1])
    for k in range(2):
        fact_in[k] = load_factors(k)
    for a in ORDER[2:]:
        for k in range(2):
            left_in[k, a] = load_left(k, a)
    mom1_in = load([(first_moment, mom1)], mom1)
    mom2_in = load([(second_moment, mom2)], mom2)
    wts_in = load([(weights, wts)], wts)

    barrier = pltpu.get_barrier_semaphore()
    fs_peers = [
        {Z: lax.rem(z + dz, 4), X: lax.rem(x + dx, 4)} for dz in range(4) for dx in range(4) if dz or dx
    ]
    tp_peers = [
        {Y: lax.rem(y + dy, 4), C: lax.rem(c + dc, 2)} for dy in range(4) for dc in range(2) if dy or dc
    ]
    for peer in fs_peers + tp_peers:
        pl.semaphore_signal(barrier, inc=1, device_id=peer, device_id_type=MESH)

    copies = Copies(send_sems, recv_sems)
    top, bottom = pl.ds(0, 128), pl.ds(128, 128)

    def transpose_right(k):
        right_in[k].wait()
        for start in range(0, 2560, 256):
            right_t[k, :, start : start + 256] = right[k, start : start + 256, :].T

    def local_grad(k, a):
        left_in[k, a].wait()
        value = jnp.dot(right_t[k], left[k, a], preferred_element_type=F32)
        for b in range(4):
            grad[k, a, b] = value[:, 128 * b : 128 * b + 128]

    def local_low(k, a):
        total = None
        for b in range(4):
            block = grad[k, a, b]
            rows = fact[k, a, 128 * b : 128 * b + 128, :]
            for part in halves(block, 2):
                term = jnp.dot(part, rows, preferred_element_type=F32)
                total = term if total is None else total + term
        if a == ORDER[0]:
            low_t[k] = total
        else:
            low_t[k] = low_t[k] + total

    pending = {}

    def one_start(k, a):
        axis = axes[k][0]
        got = {}
        got["a0"] = copies.send(grad.at[k, a, 2, top], one_a.at[k, a, 0], near(axis, 1))
        got["a1"] = copies.send(grad.at[k, a, 2, bottom], one_a.at[k, a, 1], near(axis, 3))
        got["b01"] = copies.send(grad.at[k, a, 1, bottom], one_b.at[k, a, 0, 1], near(axis, 1))
        got["b10"] = copies.send(grad.at[k, a, 3, top], one_b.at[k, a, 1, 0], near(axis, 3))
        pending["one", k, a] = got

    def one_forward(k, a):
        axis = axes[k][0]
        got = pending["one", k, a]
        got["a0"].wait_recv()
        grad[k, a, 1, 0:128] = grad[k, a, 1, 0:128] + one_a[k, a, 0]
        got["b00"] = copies.send(grad.at[k, a, 1, top], one_b.at[k, a, 0, 0], near(axis, 1))
        got["a1"].wait_recv()
        grad[k, a, 3, 128:256] = grad[k, a, 3, 128:256] + one_a[k, a, 1]
        got["b11"] = copies.send(grad.at[k, a, 3, bottom], one_b.at[k, a, 1, 1], near(axis, 3))

    def one_finish(k, a):
        got = pending["one", k, a]
        got["b01"].wait_recv()
        got["b10"].wait_recv()
        got["b00"].wait_recv()
        grad[k, a, 0, 0:128] = grad[k, a, 0, 0:128] + (one_b[k, a, 0, 0] + one_b[k, a, 1, 0])
        got["b11"].wait_recv()
        grad[k, a, 0, 128:256] = grad[k, a, 0, 128:256] + (one_b[k, a, 0, 1] + one_b[k, a, 1, 1])

    def two_start(k):
        axis = axes[k][1]
        got = pending["two", k] = {}
        got["a0"] = copies.send(grad.at[k, 2, 0, top], two_a.at[k, 0], near(axis, 1))
        got["a1"] = copies.send(grad.at[k, 2, 0, bottom], two_a.at[k, 1], near(axis, 3))

    def two_plus(k):
        axis = axes[k][1]
        got = pending["two", k]
        got["b01"] = copies.send(grad.at[k, 1, 0, bottom], two_b.at[k, 0, 1], near(axis, 1))
        got["a0"].wait_recv()
        grad[k, 1, 0, 0:128] = grad[k, 1, 0, 0:128] + two_a[k, 0]
        got["b00"] = copies.send(grad.at[k, 1, 0, top], two_b.at[k, 0, 0], near(axis, 1))

    def two_minus(k):
        axis = axes[k][1]
        got = pending["two", k]
        got["b10"] = copies.send(grad.at[k, 3, 0, top], two_b.at[k, 1, 0], near(axis, 3))
        got["a1"].wait_recv()
        grad[k, 3, 0, 128:256] = grad[k, 3, 0, 128:256] + two_a[k, 1]
        got["b11"] = copies.send(grad.at[k, 3, 0, bottom], two_b.at[k, 1, 1], near(axis, 3))

    def two_finish(k):
        got = pending["two", k]
        for name in ("b01", "b10", "b00", "b11"):
            got[name].wait_recv()
        top_sum = grad[k, 0, 0, 0:128] + (two_b[k, 0, 0] + two_b[k, 1, 0])
        bottom_sum = grad[k, 0, 0, 128:256] + (two_b[k, 0, 1] + two_b[k, 1, 1])
        return jnp.concatenate([top_sum, bottom_sum], axis=0)

    def low_rows(k, b, half=None):
        start = lax.rem(coord[axes[k][0]] + b, 4) * 64
        if half is None:
            return pl.ds(pl.multiple_of(start, 64), 64)
        return pl.ds(pl.multiple_of(start + 32 * half, 32), 32)

    def low_piece(k, a):
        first, second = axes[k]
        return pl.ds(pl.multiple_of(coord[first] * 64 + lax.rem(coord[second] + a, 4) * 16, 16), 16)

    def low_start(k):
        axis = axes[k][0]
        got = pending["low", k] = {}
        got["a0"] = copies.send(low_t.at[k, low_rows(k, 2, 0)], low_a.at[k, 0], near(axis, 1))
        got["a1"] = copies.send(low_t.at[k, low_rows(k, 2, 1)], low_a.at[k, 1], near(axis, 3))
        got["b01"] = copies.send(low_t.at[k, low_rows(k, 1, 1)], low_b.at[k, 0, 1], near(axis, 1))
        got["b10"] = copies.send(low_t.at[k, low_rows(k, 3, 0)], low_b.at[k, 1, 0], near(axis, 3))

    def low_forward(k):
        axis = axes[k][0]
        got = pending["low", k]
        got["a0"].wait_recv()
        rows = low_rows(k, 1, 0)
        low_t[k, rows] = low_t[k, rows] + low_a[k, 0]
        got["b00"] = copies.send(low_t.at[k, rows], low_b.at[k, 0, 0], near(axis, 1))
        got["a1"].wait_recv()
        rows = low_rows(k, 3, 1)
        low_t[k, rows] = low_t[k, rows] + low_a[k, 1]
        got["b11"] = copies.send(low_t.at[k, rows], low_b.at[k, 1, 1], near(axis, 3))

    def low_second(k):
        got = pending["low", k]
        for name in ("b01", "b10", "b00", "b11"):
            got[name].wait_recv()
        for half in range(2):
            rows = low_rows(k, 0, half)
            low_t[k, rows] = low_t[k, rows] + (low_b[k, 0, half] + low_b[k, 1, half])
        pending["low2", k] = [
            copies.send(low_t.at[k, low_piece(k, a)], low_in.at[k, 3 - a], near(axes[k][1], a)) for a in (2, 1, 3)
        ]

    def low_third(k):
        for copy in pending["low2", k]:
            copy.wait_recv()
        rows = low_piece(k, 0)
        low_all[k, rows] = low_t[k, rows] + low_in[k, 0] + low_in[k, 1] + low_in[k, 2]
        pending["low3", k] = [
            copies.send(low_all.at[k, rows], low_all.at[k, rows], near(axes[k][1], a)) for a in (2, 1, 3)
        ]

    def low_fourth(k):
        for copy in pending["low3", k]:
            copy.wait_recv()
        axis = axes[k][0]
        rows = low_rows(k, 0)
        got = pending["low4", k] = {}
        got["plus"] = copies.send(low_all.at[k, rows], low_all.at[k, rows], near(axis, 1))
        got["minus"] = copies.send(low_all.at[k, rows], low_all.at[k, rows], near(axis, 3))

    def low_fifth(k):
        axis = axes[k][0]
        got = pending["low4", k]
        got["plus"].wait_recv()
        rows = low_rows(k, 3, 0)
        got["far0"] = copies.send(low_all.at[k, rows], low_all.at[k, rows], near(axis, 1))
        got["minus"].wait_recv()
        rows = low_rows(k, 1, 1)
        got["far1"] = copies.send(low_all.at[k, rows], low_all.at[k, rows], near(axis, 3))

    def moments(k):
        pending["low4", k]["far0"].wait_recv()
        pending["low4", k]["far1"].wait_recv()
        low = low_all[k].T
        first = 0.9 * mom1[k] + 0.1 * low
        second = 0.95 * mom2[k] + 0.05 * low * low
        out_1[k] = first
        out_2[k] = second
        normed = first / (jnp.sqrt(second) + 1e-06)
        tp_own[k] = folded(normed * normed)
        tp_own[2 + k] = folded(low * low)
        mine = fact[k, 0, 0:128, :]
        own_p[k] = sum(jnp.dot(mine, part, preferred_element_type=F32) for part in halves(normed, 3))
        own_f[k] = sum(jnp.dot(mine, part, preferred_element_type=F32) for part in halves(low, 3))

    both = range(2)
    c0, c1, c2, c3 = ORDER
    for k in both:
        transpose_right(k)
        local_grad(k, c0)
        if k == 0:
            pl.semaphore_wait(barrier, len(fs_peers) + len(tp_peers))
        one_start(k, c0)
    for k in both:
        fact_in[k].wait()
        local_low(k, c0)
    for k in both:
        local_grad(k, c1)
        one_forward(k, c0)
        one_start(k, c1)
    for k in both:
        local_low(k, c1)
        local_grad(k, c2)
    for k in both:
        local_low(k, c2)
        local_grad(k, c3)
        one_forward(k, c1)
        one_start(k, c2)
    for k in both:
        local_low(k, c3)
        low_start(k)
    for k in both:
        one_finish(k, c0)
        two_start(k)
    for k in both:
        one_forward(k, c2)
    for k in both:
        low_forward(k)
        one_start(k, c3)
    for k in both:
        one_finish(k, c1)
        two_plus(k)
    for k in both:
        low_second(k)
    for k in both:
        one_forward(k, c3)
    for k in both:
        low_third(k)
    for k in both:
        one_finish(k, c2)
        two_minus(k)
    for k in both:
        low_fourth(k)
    for k in both:
        one_finish(k, c3)
    for k in both:
        low_fifth(k)
    mom1_in.wait()
    mom2_in.wait()
    wts_in.wait()
    for k in both:
        moments(k)
    tp_copies = [copies.send(tp_own, tp_in.at[i], peer) for i, peer in enumerate(tp_peers)]
    tot_own[6:8, :] = jnp.zeros((2, 128), F32)
    for k in both:
        resid = two_finish(k).T - own_f[k]
        own_f[k] = resid
        parts = (own_p[k] * own_p[k], own_p[k] * resid, resid * resid)
        for i, part in enumerate(parts):
            tot_own[3 * k + i : 3 * k + i + 1, :] = folded(part).sum(axis=0, keepdims=True)
    tot_copies = [copies.send(tot_own, tot_in.at[i], peer) for i, peer in enumerate(fs_peers)]
    for copy in tp_copies:
        copy.wait_recv()
    sums = tp_own[...]
    for i in range(len(tp_peers)):
        sums = sums + tp_in[i]
    ratios = [
        jnp.sqrt(jnp.sum(sums[k], keepdims=True)) / jnp.sqrt(jnp.sum(sums[2 + k], keepdims=True) + 1e-06)
        for k in both
    ]
    for k in both:
        out_u[k] = own_p[k] + ratios[k] * own_f[k]
    for copy in tot_copies:
        copy.wait_recv()
    parts = tot_own[...]
    for i in range(len(fs_peers)):
        parts = parts + tot_in[i]
    last_own[...] = parts
    last_copies = [copies.send(last_own, last_in.at[i], peer) for i, peer in enumerate(tp_peers)]
    for copy in last_copies:
        copy.wait_recv()
    for i in range(len(tp_peers)):
        parts = parts + last_in[i]
    total = None
    for k in both:
        square = parts[3 * k : 3 * k + 1]
        square = square + ratios[k] * (2.0 * parts[3 * k + 1 : 3 * k + 2] + ratios[k] * parts[3 * k + 2 : 3 * k + 3])
        total = square if total is None else total + square
    scale = lax.rsqrt(jnp.sum(total, keepdims=True) / (2.0 * 2048 * 2048) + 1e-06)

    for k in range(2):
        value = out_u[k] * scale
        out_u[k] = value
        value = wts[k] - 0.02 * value
        out_w[k] = value
        gathered[k, 0, 0] = value.astype(BF16)

    upper, lower = pl.ds(0, 64), pl.ds(64, 64)

    def spread(k, b):
        block = gathered.at[k, 0, b]
        got = pending["w", k, b] = {}
        got["plus"] = copies.send(block, gathered.at[k, 3, b], near(axes[k][1], 1))
        got["minus"] = copies.send(block, gathered.at[k, 1, b], near(axes[k][1], 3))

    def relay(k, b):
        got = pending["w", k, b]
        got["plus"].wait_recv()
        got["far0"] = copies.send(gathered.at[k, 3, b, upper], gathered.at[k, 2, b, upper], near(axes[k][1], 1))
        got["minus"].wait_recv()
        got["far1"] = copies.send(gathered.at[k, 1, b, lower], gathered.at[k, 2, b, lower], near(axes[k][1], 3))

    def land(k, b):
        got = pending["w", k, b]
        got["far0"].wait_recv()
        got["far1"].wait_recv()

    for k in range(2):
        axis = axes[k][0]
        got = pending["v", k] = {}
        got["plus"] = copies.send(gathered.at[k, 0, 0], gathered.at[k, 0, 3], near(axis, 1))
        got["minus"] = copies.send(gathered.at[k, 0, 0], gathered.at[k, 0, 1], near(axis, 3))
    for k in range(2):
        spread(k, 0)
    for k in range(2):
        axis = axes[k][0]
        got = pending["v", k]
        got["plus"].wait_recv()
        got["far0"] = copies.send(gathered.at[k, 0, 3, upper], gathered.at[k, 0, 2, upper], near(axis, 1))
        got["minus"].wait_recv()
        got["far1"] = copies.send(gathered.at[k, 0, 1, lower], gathered.at[k, 0, 2, lower], near(axis, 3))
        spread(k, 3)
        spread(k, 1)
    for k in range(2):
        relay(k, 0)
    for k in range(2):
        got = pending["v", k]
        got["far0"].wait_recv()
        got["far1"].wait_recv()
        spread(k, 2)
    for b in (3, 1, 2):
        for k in range(2):
            relay(k, b)
    for b in (0, 3, 1, 2):
        for k in range(2):
            land(k, b)
    for copy in copies.made:
        copy.wait_send()


def write_out(
    out_w, out_u, out_1, out_2, gathered, new_weights, update, new_first, new_second, weight_copy, sems
):
    z, x = lax.axis_index(Z), lax.axis_index(X)
    pairs = []
    for a in range(4):
        for b in range(4):
            for k in range(2):
                dz, dx = (a, b) if k == 0 else (b, a)
                block = lax.rem(z + dz, 4) * 4 + lax.rem(x + dx, 4)
                rows = pl.ds(pl.multiple_of(block * 128, 128), 128)
                pairs.append((gathered.at[k, a, b], weight_copy.at[k, rows, :]))
    pairs += [(out_1, new_first), (out_2, new_second), (out_w, new_weights), (out_u, update)]
    copies = [pltpu.make_async_copy(*pair, sems.at[i]) for i, pair in enumerate(pairs)]
    for copy in copies:
        copy.start()
    for copy in copies:
        copy.wait()


def per_device(*args):
    any_space = pl.BlockSpec(memory_space=pl.ANY)
    vmem_space = pl.BlockSpec(memory_space=pltpu.VMEM)
    held = (
        ((2, 128, 256), F32),
        ((2, 128, 256), F32),
        ((2, 256, 256), F32),
        ((2, 256, 256), F32),
        ((2, 4, 4, 128, 256), BF16),
    )
    dma = pltpu.SemaphoreType.DMA
    results = pl.pallas_call(
        kernel,
        name="step",
        out_shape=[pltpu.VMEM(*shape) for shape in held],
        in_specs=[any_space] * 8,
        out_specs=[vmem_space] * 5,
        scratch_shapes=[
            pltpu.VMEM((2, 4, 2560, 512), BF16),
            pltpu.VMEM((2, 2560, 256), BF16),
            pltpu.VMEM((2, 256, 2560), BF16),
            pltpu.VMEM((2, 4, 512, 256), BF16),
            pltpu.VMEM((2, 4, 4, 256, 128), F32),
            pltpu.VMEM((2, 4, 2, 128, 128), F32),
            pltpu.VMEM((2, 4, 2, 2, 128, 128), F32),
            pltpu.VMEM((2, 2, 128, 128), F32),
            pltpu.VMEM((2, 2, 2, 128, 128), F32),
            pltpu.VMEM((2, 256, 256), F32),
            pltpu.VMEM((2, 2, 32, 256), F32),
            pltpu.VMEM((2, 2, 2, 32, 256), F32),
            pltpu.VMEM((2, 3, 16, 256), F32),
            pltpu.VMEM((2, 256, 256), F32),
            pltpu.VMEM((2, 128, 256), F32),
            pltpu.VMEM((2, 256, 256), F32),
            pltpu.VMEM((2, 256, 256), F32),
            pltpu.VMEM((2, 128, 256), F32),
            pltpu.VMEM((2, 128, 256), F32),
            pltpu.VMEM((4, 8, 128), F32),
            pltpu.VMEM((7, 4, 8, 128), F32),
            pltpu.VMEM((8, 128), F32),
            pltpu.VMEM((15, 8, 128), F32),
            pltpu.VMEM((8, 128), F32),
            pltpu.VMEM((7, 8, 128), F32),
            dma((LOADS,)),
            dma((COPIES,)),
            dma((COPIES,)),
        ],
        compiler_params=pltpu.CompilerParams(
            collective_id=0, has_side_effects=True, vmem_limit_bytes=60 * 1024 * 1024
        ),
    )(*args)
    return pl.pallas_call(
        write_out,
        name="write_out",
        out_shape=[jax.ShapeDtypeStruct(shape, kind) for shape, kind in held[:4]]
        + [jax.ShapeDtypeStruct((2, 2048, 256), BF16)],
        in_specs=[vmem_space] * 5,
        out_specs=[any_space] * 5,
        scratch_shapes=[dma((36,))],
        compiler_params=pltpu.CompilerParams(vmem_limit_bytes=1024 * 1024),
    )(*results)


def solution(mesh):
    finer = Mesh(mesh.devices.reshape(4, 4, 4, 2), (Z, X, Y, C))
    in_specs = (
        P(FS, None),
        P(FS, None),
        P(FS, TP),
        P(FS, TP),
        P(None, FS, TP),
        P(),
        P(None, None, TP),
        P(None, None, TP),
    )
    out_specs = (
        P(None, FS, TP),
        P(None, FS, TP),
        P(None, None, TP),
        P(None, None, TP),
        P(None, None, TP),
    )
    return jax.shard_map(per_device, mesh=finer, in_specs=in_specs, out_specs=out_specs, check_vma=False)
```

```python
import math

import jax
import jax.numpy as jnp
from jax import lax
from jax.experimental import pallas as pl
from jax.experimental.pallas import tpu as pltpu
from jax.sharding import Mesh
from jax.sharding import PartitionSpec as P

Z, X, Y, C = "fs_0", "fs_1", "tp_0", "tp_1"
FS, TP = (Z, X), (Y, C)
MESH = pl.DeviceIdType.MESH
F32, BF16 = jnp.float32, jnp.bfloat16
ORDER = (2, 1, 3, 0)


class Copies:
    def __init__(self, send_sems, recv_sems, spare):
        self.send_sems, self.recv_sems, self.spare = send_sems, recv_sems, spare
        self.landings, self.sent = 0, [0]

    def landing(self):
        self.landings += 1
        return self.landings - 1

    def send(self, src, dst, device, landing):
        size = math.prod(src.shape) * src.dtype.itemsize // 1024
        if self.sent[-1] + size > self.spare.shape[0]:
            self.sent.append(0)
        self.sent[-1] += size
        pltpu.make_async_remote_copy(
            src_ref=src,
            dst_ref=dst,
            send_sem=self.send_sems.at[len(self.sent) - 1],
            recv_sem=self.recv_sems.at[landing],
            device_id=device,
            device_id_type=MESH,
        ).start()

    def wait(self, landing, place):
        pltpu.make_async_copy(place, place, self.recv_sems.at[landing]).wait()

    def wait_sent(self):
        for index, size in enumerate(self.sent):
            rows = self.spare.at[pl.ds(0, size)]
            pltpu.make_async_copy(rows, rows, self.send_sems.at[index]).wait()


SENDS, LANDINGS, LOADS = 3, 73, 15


def halves(value, terms):
    out = []
    for _ in range(terms - 1):
        part = value.astype(BF16)
        out.append(part)
        value = value - part.astype(F32)
    out.append(value.astype(BF16))
    return out


def folded(value):
    rows, cols = value.shape
    total = value[:, 0:128]
    for start in range(128, cols, 128):
        total = total + value[:, start : start + 128]
    return total.reshape(rows // 8, 8, 128).sum(axis=0)


def kernel(
    layer_inputs, output_cot, query_cot, head_outputs, weights, factors, first_moment, second_moment,
    out_w, out_u, out_1, out_2, gathered,
    left, right, right_t, fact, grad, one_a, one_b, two_a, two_b,
    low_t, low_a, low_b, low_in, low_all, wts, mom1, mom2,
    own_p, own_f, tp_own, tp_in, tot_own, tot_in, last_own, last_in,
    load_sems, send_sems, recv_sems,
):
    z, x, y, c = (lax.axis_index(name) for name in (Z, X, Y, C))
    lefts, rights = (layer_inputs, output_cot), (query_cot, head_outputs)
    coord = {Z: z, X: x, Y: y, C: c}
    axes = ((X, Z), (Z, X))

    def near(axis, delta):
        return {axis: lax.rem(coord[axis] + delta, 4)}

    def place(k, a, b):
        first, second = axes[k]
        at = {first: lax.rem(coord[first] + b, 4), second: lax.rem(coord[second] + a, 4)}
        return at[Z] * 4 + at[X]

    loads = []

    def load(pairs, whole):
        sem = load_sems.at[len(loads)]
        for src, dst in pairs:
            pltpu.make_async_copy(src, dst, sem).start()
        loads.append(pltpu.make_async_copy(whole, whole, sem))
        return loads[-1]

    def load_left(k, a):
        pairs = []
        for b in range(4):
            cols = pl.ds(pl.multiple_of(place(k, a, b) * 128, 128), 128)
            pairs.append((lefts[k].at[:, cols], left.at[k, a, :, pl.ds(128 * b, 128)]))
        return load(pairs, left.at[k, a])

    def load_factors(k):
        pairs = []
        for a in range(4):
            for b in range(4):
                rows = pl.ds(pl.multiple_of(place(k, a, b) * 128, 128), 128)
                pairs.append((factors.at[k, rows, :], fact.at[k, a, pl.ds(128 * b, 128), :]))
        return load(pairs, fact.at[k])

    right_in, left_in, fact_in = [None] * 2, {}, [None] * 2
    for k in range(2):
        right_in[k] = load([(rights[k], right.at[k])], right.at[k])
        left_in[k, ORDER[0]] = load_left(k, ORDER[0])
    for k in range(2):
        left_in[k, ORDER[1]] = load_left(k, ORDER[1])
    for k in range(2):
        fact_in[k] = load_factors(k)
    for a in ORDER[2:]:
        for k in range(2):
            left_in[k, a] = load_left(k, a)
    mom1_in = load([(first_moment, mom1)], mom1)
    mom2_in = load([(second_moment, mom2)], mom2)
    wts_in = load([(weights, wts)], wts)

    barrier = pltpu.get_barrier_semaphore()
    fs_peers = [
        {Z: lax.rem(z + dz, 4), X: lax.rem(x + dx, 4)} for dz in range(4) for dx in range(4) if dz or dx
    ]
    tp_peers = [
        {Y: lax.rem(y + dy, 4), C: lax.rem(c + dc, 2)} for dy in range(4) for dc in range(2) if dy or dc
    ]
    for peer in fs_peers + tp_peers:
        pl.semaphore_signal(barrier, inc=1, device_id=peer, device_id_type=MESH)

    copies = Copies(send_sems, recv_sems, left.at[0, 0])
    top, bottom = pl.ds(0, 128), pl.ds(128, 128)

    def transpose_right(k):
        right_in[k].wait()
        for start in range(0, 2560, 256):
            right_t[k, :, start : start + 256] = right[k, start : start + 256, :].T

    def local_grad(k, a):
        left_in[k, a].wait()
        value = jnp.dot(right_t[k], left[k, a], preferred_element_type=F32)
        for b in range(4):
            grad[k, a, b] = value[:, 128 * b : 128 * b + 128]

    def local_low(k, a):
        total = None
        value = jnp.concatenate([grad[k, a, b] for b in range(4)], axis=1)
        for part in halves(value, 2):
            term = jnp.dot(part, fact[k, a], preferred_element_type=F32)
            total = term if total is None else total + term
        if a == ORDER[0]:
            low_t[k] = total
        else:
            low_t[k] = low_t[k] + total

    pending = {}

    def opening(key, axis, far, minus, plus, into_a, into_b):
        marks = pending[key] = [copies.landing() for _ in range(3)]
        copies.send(far[0], into_a.at[0], near(axis, 1), marks[0])
        copies.send(far[1], into_a.at[1], near(axis, 3), marks[1])
        copies.send(plus[1], into_b.at[0, 1], near(axis, 1), marks[2])
        copies.send(minus[0], into_b.at[1, 0], near(axis, 3), marks[2])

    def one_start(k, a):
        far, plus, minus = ((grad.at[k, a, b, top], grad.at[k, a, b, bottom]) for b in (2, 1, 3))
        opening(("one", k, a), axes[k][0], far, minus, plus, one_a.at[k, a], one_b.at[k, a])

    def one_forward(k, a):
        axis, marks = axes[k][0], pending["one", k, a]
        copies.wait(marks[0], one_a.at[k, a, 0])
        grad[k, a, 1, 0:128] = grad[k, a, 1, 0:128] + one_a[k, a, 0]
        copies.send(grad.at[k, a, 1, top], one_b.at[k, a, 0, 0], near(axis, 1), marks[2])
        copies.wait(marks[1], one_a.at[k, a, 1])
        grad[k, a, 3, 128:256] = grad[k, a, 3, 128:256] + one_a[k, a, 1]
        copies.send(grad.at[k, a, 3, bottom], one_b.at[k, a, 1, 1], near(axis, 3), marks[2])

    def one_finish(k, a):
        copies.wait(pending["one", k, a][2], one_b.at[k, a])
        grad[k, a, 0, 0:128] = grad[k, a, 0, 0:128] + (one_b[k, a, 0, 0] + one_b[k, a, 1, 0])
        grad[k, a, 0, 128:256] = grad[k, a, 0, 128:256] + (one_b[k, a, 0, 1] + one_b[k, a, 1, 1])

    def two_start(k):
        axis = axes[k][1]
        marks = pending["two", k] = [copies.landing() for _ in range(3)]
        copies.send(grad.at[k, 2, 0, top], two_a.at[k, 0], near(axis, 1), marks[0])
        copies.send(grad.at[k, 2, 0, bottom], two_a.at[k, 1], near(axis, 3), marks[1])

    def two_plus(k):
        axis, marks = axes[k][1], pending["two", k]
        copies.send(grad.at[k, 1, 0, bottom], two_b.at[k, 0, 1], near(axis, 1), marks[2])
        copies.wait(marks[0], two_a.at[k, 0])
        grad[k, 1, 0, 0:128] = grad[k, 1, 0, 0:128] + two_a[k, 0]
        copies.send(grad.at[k, 1, 0, top], two_b.at[k, 0, 0], near(axis, 1), marks[2])

    def two_minus(k):
        axis, marks = axes[k][1], pending["two", k]
        copies.send(grad.at[k, 3, 0, top], two_b.at[k, 1, 0], near(axis, 3), marks[2])
        copies.wait(marks[1], two_a.at[k, 1])
        grad[k, 3, 0, 128:256] = grad[k, 3, 0, 128:256] + two_a[k, 1]
        copies.send(grad.at[k, 3, 0, bottom], two_b.at[k, 1, 1], near(axis, 3), marks[2])

    def two_finish(k):
        copies.wait(pending["two", k][2], two_b.at[k])
        top_sum = grad[k, 0, 0, 0:128] + (two_b[k, 0, 0] + two_b[k, 1, 0])
        bottom_sum = grad[k, 0, 0, 128:256] + (two_b[k, 0, 1] + two_b[k, 1, 1])
        return jnp.concatenate([top_sum, bottom_sum], axis=0)

    def low_rows(k, b, half=None):
        start = lax.rem(coord[axes[k][0]] + b, 4) * 64
        if half is None:
            return pl.ds(pl.multiple_of(start, 64), 64)
        return pl.ds(pl.multiple_of(start + 32 * half, 32), 32)

    def low_piece(k, a):
        first, second = axes[k]
        return pl.ds(pl.multiple_of(coord[first] * 64 + lax.rem(coord[second] + a, 4) * 16, 16), 16)

    def low_start(k):
        far, plus, minus = ([low_t.at[k, low_rows(k, b, half)] for half in range(2)] for b in (2, 1, 3))
        opening(("low", k), axes[k][0], far, minus, plus, low_a.at[k], low_b.at[k])

    def low_forward(k):
        axis, marks = axes[k][0], pending["low", k]
        copies.wait(marks[0], low_a.at[k, 0])
        rows = low_rows(k, 1, 0)
        low_t[k, rows] = low_t[k, rows] + low_a[k, 0]
        copies.send(low_t.at[k, rows], low_b.at[k, 0, 0], near(axis, 1), marks[2])
        copies.wait(marks[1], low_a.at[k, 1])
        rows = low_rows(k, 3, 1)
        low_t[k, rows] = low_t[k, rows] + low_a[k, 1]
        copies.send(low_t.at[k, rows], low_b.at[k, 1, 1], near(axis, 3), marks[2])

    def low_second(k):
        copies.wait(pending["low", k][2], low_b.at[k])
        for half in range(2):
            rows = low_rows(k, 0, half)
            low_t[k, rows] = low_t[k, rows] + (low_b[k, 0, half] + low_b[k, 1, half])
        mark = pending["low2", k] = copies.landing()
        for a in (2, 1, 3):
            copies.send(low_t.at[k, low_piece(k, a)], low_in.at[k, 3 - a], near(axes[k][1], a), mark)

    def low_third(k):
        copies.wait(pending["low2", k], low_in.at[k])
        rows = low_piece(k, 0)
        low_all[k, rows] = low_t[k, rows] + low_in[k, 0] + low_in[k, 1] + low_in[k, 2]
        mark = pending["low3", k] = copies.landing()
        for peer in fs_peers:
            copies.send(low_all.at[k, rows], low_all.at[k, rows], peer, mark)

    def moments(k):
        copies.wait(pending["low3", k], low_all.at[k, pl.ds(0, 240)])
        low = low_all[k].T
        first = 0.9 * mom1[k] + 0.1 * low
        second = 0.95 * mom2[k] + 0.05 * low * low
        out_1[k] = first
        out_2[k] = second
        normed = first / (jnp.sqrt(second) + 1e-06)
        tp_own[k] = folded(normed * normed)
        tp_own[2 + k] = folded(low * low)
        mine = fact[k, 0, 0:128, :]
        own_p[k] = sum(jnp.dot(mine, part, preferred_element_type=F32) for part in halves(normed, 3))
        own_f[k] = sum(jnp.dot(mine, part, preferred_element_type=F32) for part in halves(low, 3))

    both = range(2)
    c0, c1, c2, c3 = ORDER
    for k in both:
        transpose_right(k)
        local_grad(k, c0)
        if k == 0:
            pl.semaphore_wait(barrier, len(fs_peers) + len(tp_peers))
        one_start(k, c0)
    for k in both:
        local_grad(k, c1)
    for k in both:
        fact_in[k].wait()
        local_low(k, c0)
        one_forward(k, c0)
        one_start(k, c1)
    for k in both:
        local_low(k, c1)
    for k in both:
        local_grad(k, c2)
        local_low(k, c2)
        one_forward(k, c1)
    for k in both:
        local_grad(k, c3)
        local_low(k, c3)
        low_start(k)
        one_start(k, c2)
    for k in both:
        one_finish(k, c0)
        two_start(k)
    for k in both:
        low_forward(k)
    for k in both:
        one_forward(k, c2)
    for k in both:
        low_second(k)
    for k in both:
        one_start(k, c3)
    for k in both:
        one_finish(k, c1)
        two_plus(k)
    for k in both:
        low_third(k)
        one_forward(k, c3)
    for k in both:
        one_finish(k, c2)
        two_minus(k)
    for k in both:
        one_finish(k, c3)
    mom1_in.wait()
    mom2_in.wait()
    wts_in.wait()
    for k in both:
        moments(k)
    tp_mark, tot_mark, last_mark = (copies.landing() for _ in range(3))
    for i, peer in enumerate(tp_peers):
        copies.send(tp_own, tp_in.at[i], peer, tp_mark)
    tot_own[6:8, :] = jnp.zeros((2, 128), F32)
    for k in both:
        resid = two_finish(k).T - own_f[k]
        own_f[k] = resid
        parts = (own_p[k] * own_p[k], own_p[k] * resid, resid * resid)
        for i, part in enumerate(parts):
            tot_own[3 * k + i : 3 * k + i + 1, :] = folded(part).sum(axis=0, keepdims=True)
    for i, peer in enumerate(fs_peers):
        copies.send(tot_own, tot_in.at[i], peer, tot_mark)
    copies.wait(tp_mark, tp_in)
    sums = tp_own[...]
    for i in range(len(tp_peers)):
        sums = sums + tp_in[i]
    ratios = [
        jnp.sqrt(jnp.sum(sums[k], keepdims=True)) / jnp.sqrt(jnp.sum(sums[2 + k], keepdims=True) + 1e-06)
        for k in both
    ]
    for k in both:
        out_u[k] = own_p[k] + ratios[k] * own_f[k]
    copies.wait(tot_mark, tot_in)
    parts = tot_own[...]
    for i in range(len(fs_peers)):
        parts = parts + tot_in[i]
    last_own[...] = parts
    for i, peer in enumerate(tp_peers):
        copies.send(last_own, last_in.at[i], peer, last_mark)
    copies.wait(last_mark, last_in)
    for i in range(len(tp_peers)):
        parts = parts + last_in[i]
    total = None
    for k in both:
        square = parts[3 * k : 3 * k + 1]
        square = square + ratios[k] * (2.0 * parts[3 * k + 1 : 3 * k + 2] + ratios[k] * parts[3 * k + 2 : 3 * k + 3])
        total = square if total is None else total + square
    scale = lax.rsqrt(jnp.sum(total, keepdims=True) / (2.0 * 2048 * 2048) + 1e-06)

    for k in range(2):
        value = out_u[k] * scale
        out_u[k] = value
        value = wts[k] - 0.02 * value
        out_w[k] = value
        gathered[k, 0, 0] = value.astype(BF16)

    upper, lower = pl.ds(0, 64), pl.ds(64, 64)

    def spread(k, b):
        marks = pending["w", k, b] = [copies.landing() for _ in range(3)]
        copies.send(gathered.at[k, 0, b], gathered.at[k, 3, b], near(axes[k][1], 1), marks[0])
        copies.send(gathered.at[k, 0, b], gathered.at[k, 1, b], near(axes[k][1], 3), marks[1])

    def relay(k, b):
        marks = pending["w", k, b]
        copies.wait(marks[0], gathered.at[k, 3, b])
        copies.send(gathered.at[k, 3, b, upper], gathered.at[k, 2, b, upper], near(axes[k][1], 1), marks[2])
        copies.wait(marks[1], gathered.at[k, 1, b])
        copies.send(gathered.at[k, 1, b, lower], gathered.at[k, 2, b, lower], near(axes[k][1], 3), marks[2])

    def land(k, b):
        copies.wait(pending["w", k, b][2], gathered.at[k, 2, b])

    def v_start(k):
        marks = pending["v", k] = [copies.landing() for _ in range(3)]
        copies.send(gathered.at[k, 0, 0], gathered.at[k, 0, 3], near(axes[k][0], 1), marks[0])
        copies.send(gathered.at[k, 0, 0], gathered.at[k, 0, 1], near(axes[k][0], 3), marks[1])

    def v_forward(k):
        marks = pending["v", k]
        copies.wait(marks[0], gathered.at[k, 0, 3])
        copies.send(gathered.at[k, 0, 3, upper], gathered.at[k, 0, 2, upper], near(axes[k][0], 1), marks[2])
        copies.wait(marks[1], gathered.at[k, 0, 1])
        copies.send(gathered.at[k, 0, 1, lower], gathered.at[k, 0, 2, lower], near(axes[k][0], 3), marks[2])

    def v_finish(k):
        copies.wait(pending["v", k][2], gathered.at[k, 0, 2])

    for k in both:
        v_start(k)
    for k in both:
        spread(k, 0)
    for k in both:
        v_forward(k)
        spread(k, 3)
        spread(k, 1)
    for k in both:
        relay(k, 0)
    for k in both:
        v_finish(k)
        spread(k, 2)
    for b in (3, 1, 2):
        for k in both:
            relay(k, b)
    for b in (0, 3, 1, 2):
        for k in both:
            land(k, b)
    copies.wait_sent()


def write_out(
    out_w, out_u, out_1, out_2, gathered, new_weights, update, new_first, new_second, weight_copy, sems
):
    z, x = lax.axis_index(Z), lax.axis_index(X)
    pairs = []
    for a in range(4):
        for b in range(4):
            for k in range(2):
                dz, dx = (a, b) if k == 0 else (b, a)
                block = lax.rem(z + dz, 4) * 4 + lax.rem(x + dx, 4)
                rows = pl.ds(pl.multiple_of(block * 128, 128), 128)
                pairs.append((gathered.at[k, a, b], weight_copy.at[k, rows, :]))
    for src, dst in pairs:
        pltpu.make_async_copy(src, dst, sems.at[0]).start()
    pairs = ((out_1, new_first), (out_2, new_second), (out_w, new_weights), (out_u, update))
    copies = [pltpu.make_async_copy(*pair, sems.at[1 + i]) for i, pair in enumerate(pairs)]
    for copy in copies:
        copy.start()
    for copy in copies:
        copy.wait()
    pltpu.make_async_copy(gathered, gathered, sems.at[0]).wait()


def per_device(*args):
    any_space = pl.BlockSpec(memory_space=pl.ANY)
    vmem_space = pl.BlockSpec(memory_space=pltpu.VMEM)
    held = (
        ((2, 128, 256), F32),
        ((2, 128, 256), F32),
        ((2, 256, 256), F32),
        ((2, 256, 256), F32),
        ((2, 4, 4, 128, 256), BF16),
    )
    dma = pltpu.SemaphoreType.DMA
    results = pl.pallas_call(
        kernel,
        name="step",
        out_shape=[pltpu.VMEM(*shape) for shape in held],
        in_specs=[any_space] * 8,
        out_specs=[vmem_space] * 5,
        scratch_shapes=[
            pltpu.VMEM((2, 4, 2560, 512), BF16),
            pltpu.VMEM((2, 2560, 256), BF16),
            pltpu.VMEM((2, 256, 2560), BF16),
            pltpu.VMEM((2, 4, 512, 256), BF16),
            pltpu.VMEM((2, 4, 4, 256, 128), F32),
            pltpu.VMEM((2, 4, 2, 128, 128), F32),
            pltpu.VMEM((2, 4, 2, 2, 128, 128), F32),
            pltpu.VMEM((2, 2, 128, 128), F32),
            pltpu.VMEM((2, 2, 2, 128, 128), F32),
            pltpu.VMEM((2, 256, 256), F32),
            pltpu.VMEM((2, 2, 32, 256), F32),
            pltpu.VMEM((2, 2, 2, 32, 256), F32),
            pltpu.VMEM((2, 3, 16, 256), F32),
            pltpu.VMEM((2, 256, 256), F32),
            pltpu.VMEM((2, 128, 256), F32),
            pltpu.VMEM((2, 256, 256), F32),
            pltpu.VMEM((2, 256, 256), F32),
            pltpu.VMEM((2, 128, 256), F32),
            pltpu.VMEM((2, 128, 256), F32),
            pltpu.VMEM((4, 8, 128), F32),
            pltpu.VMEM((7, 4, 8, 128), F32),
            pltpu.VMEM((8, 128), F32),
            pltpu.VMEM((15, 8, 128), F32),
            pltpu.VMEM((8, 128), F32),
            pltpu.VMEM((7, 8, 128), F32),
            dma((LOADS,)),
            dma((SENDS,)),
            dma((LANDINGS,)),
        ],
        compiler_params=pltpu.CompilerParams(
            collective_id=0, has_side_effects=True, vmem_limit_bytes=60 * 1024 * 1024
        ),
    )(*args)
    return pl.pallas_call(
        write_out,
        name="write_out",
        out_shape=[jax.ShapeDtypeStruct(shape, kind) for shape, kind in held[:4]]
        + [jax.ShapeDtypeStruct((2, 2048, 256), BF16)],
        in_specs=[vmem_space] * 5,
        out_specs=[any_space] * 5,
        scratch_shapes=[dma((5,))],
        compiler_params=pltpu.CompilerParams(vmem_limit_bytes=1024 * 1024),
    )(*results)


def solution(mesh):
    finer = Mesh(mesh.devices.reshape(4, 4, 4, 2), (Z, X, Y, C))
    in_specs = (
        P(FS, None),
        P(FS, None),
        P(FS, TP),
        P(FS, TP),
        P(None, FS, TP),
        P(),
        P(None, None, TP),
        P(None, None, TP),
    )
    out_specs = (
        P(None, FS, TP),
        P(None, FS, TP),
        P(None, None, TP),
        P(None, None, TP),
        P(None, None, TP),
    )
    return jax.shard_map(per_device, mesh=finer, in_specs=in_specs, out_specs=out_specs, check_vma=False)
```

```python
import math

import jax
import jax.numpy as jnp
from jax import lax
from jax.experimental import pallas as pl
from jax.experimental.pallas import tpu as pltpu
from jax.sharding import Mesh
from jax.sharding import PartitionSpec as P

Z, X, Y, C = "fs_0", "fs_1", "tp_0", "tp_1"
FS, TP = (Z, X), (Y, C)
MESH = pl.DeviceIdType.MESH
F32, BF16 = jnp.float32, jnp.bfloat16
ORDER = (2, 1, 3, 0)


class Copies:
    def __init__(self, send_sems, recv_sems, spare):
        self.send_sems, self.recv_sems, self.spare = send_sems, recv_sems, spare
        self.landings, self.sent = 0, [0]

    def landing(self):
        self.landings += 1
        return self.landings - 1

    def send(self, src, dst, device, landing, own=None):
        size = math.prod(src.shape) * src.dtype.itemsize // 1024
        if own is None:
            if self.sent[-1] + size > self.spare.shape[0]:
                self.sent.append(0)
            self.sent[-1] += size
        pltpu.make_async_remote_copy(
            src_ref=src,
            dst_ref=dst,
            send_sem=self.send_sems.at[len(self.sent) - 1 if own is None else own],
            recv_sem=self.recv_sems.at[landing],
            device_id=device,
            device_id_type=MESH,
        ).start()

    def wait(self, landing, place):
        pltpu.make_async_copy(place, place, self.recv_sems.at[landing]).wait()

    def wait_sent(self):
        for index, size in enumerate(self.sent):
            rows = self.spare.at[pl.ds(0, size)]
            pltpu.make_async_copy(rows, rows, self.send_sems.at[index]).wait()


SENDS, LANDINGS, LOADS = 4, 72, 15


def halves(value, terms):
    out = []
    for _ in range(terms - 1):
        part = value.astype(BF16)
        out.append(part)
        value = value - part.astype(F32)
    out.append(value.astype(BF16))
    return out


def folded(value):
    rows, cols = value.shape
    total = value[:, 0:128]
    for start in range(128, cols, 128):
        total = total + value[:, start : start + 128]
    return total.reshape(rows // 8, 8, 128).sum(axis=0)


def kernel(
    layer_inputs, output_cot, query_cot, head_outputs, weights, factors, first_moment, second_moment,
    out_w, out_u, out_1, out_2, gathered,
    left, right, right_t, fact, grad, one_a, one_b, two_a, two_b,
    low_t, low_a, low_b, low_in, low_all, wts, mom1, mom2,
    own_p, own_f, tp_own, tp_in, tot_own, tot_in,
    load_sems, send_sems, recv_sems,
):
    z, x, y, c = (lax.axis_index(name) for name in (Z, X, Y, C))
    lefts, rights = (layer_inputs, output_cot), (query_cot, head_outputs)
    coord = {Z: z, X: x, Y: y, C: c}
    axes = ((X, Z), (Z, X))

    def near(axis, delta):
        return {axis: lax.rem(coord[axis] + delta, 4)}

    def place(k, a, b):
        first, second = axes[k]
        at = {first: lax.rem(coord[first] + b, 4), second: lax.rem(coord[second] + a, 4)}
        return at[Z] * 4 + at[X]

    loads = []

    def load(pairs, whole):
        sem = load_sems.at[len(loads)]
        for src, dst in pairs:
            pltpu.make_async_copy(src, dst, sem).start()
        loads.append(pltpu.make_async_copy(whole, whole, sem))
        return loads[-1]

    def load_left(k, a):
        pairs = []
        for b in range(4):
            cols = pl.ds(pl.multiple_of(place(k, a, b) * 128, 128), 128)
            pairs.append((lefts[k].at[:, cols], left.at[k, a, :, pl.ds(128 * b, 128)]))
        return load(pairs, left.at[k, a])

    def load_factors(k):
        pairs = []
        for a in range(4):
            for b in range(4):
                rows = pl.ds(pl.multiple_of(place(k, a, b) * 128, 128), 128)
                pairs.append((factors.at[k, rows, :], fact.at[k, a, pl.ds(128 * b, 128), :]))
        return load(pairs, fact.at[k])

    right_in, left_in, fact_in = [None] * 2, {}, [None] * 2
    for k in range(2):
        right_in[k] = load([(rights[k], right.at[k])], right.at[k])
        left_in[k, ORDER[0]] = load_left(k, ORDER[0])
    for k in range(2):
        left_in[k, ORDER[1]] = load_left(k, ORDER[1])
    for k in range(2):
        fact_in[k] = load_factors(k)
    for a in ORDER[2:]:
        for k in range(2):
            left_in[k, a] = load_left(k, a)
    mom1_in = load([(first_moment, mom1)], mom1)
    mom2_in = load([(second_moment, mom2)], mom2)
    wts_in = load([(weights, wts)], wts)

    barrier = pltpu.get_barrier_semaphore()
    fs_peers = [
        {Z: lax.rem(z + dz, 4), X: lax.rem(x + dx, 4)} for dz in range(4) for dx in range(4) if dz or dx
    ]
    tp_peers = [
        {Y: lax.rem(y + dy, 4), C: lax.rem(c + dc, 2)} for dy in range(4) for dc in range(2) if dy or dc
    ]
    all_peers = [
        {Z: lax.rem(z + dz, 4), X: lax.rem(x + dx, 4), Y: lax.rem(y + dy, 4), C: lax.rem(c + dc, 2)}
        for dz in ORDER
        for dx in ORDER
        for dy in ORDER
        for dc in range(2)
        if dz or dx or dy or dc
    ]
    for peer in fs_peers + tp_peers:
        pl.semaphore_signal(barrier, inc=1, device_id=peer, device_id_type=MESH)

    copies = Copies(send_sems, recv_sems, left.at[0, 0])
    top, bottom = pl.ds(0, 128), pl.ds(128, 128)

    def transpose_right(k):
        right_in[k].wait()
        for start in range(0, 2560, 256):
            right_t[k, :, start : start + 256] = right[k, start : start + 256, :].T

    def local_grad(k, a):
        left_in[k, a].wait()
        value = jnp.dot(right_t[k], left[k, a], preferred_element_type=F32)
        for b in range(4):
            grad[k, a, b] = value[:, 128 * b : 128 * b + 128]

    def local_low(k, a):
        total = None
        value = jnp.concatenate([grad[k, a, b] for b in range(4)], axis=1)
        for part in halves(value, 2):
            term = jnp.dot(part, fact[k, a], preferred_element_type=F32)
            total = term if total is None else total + term
        if a == ORDER[0]:
            low_t[k] = total
        else:
            low_t[k] = low_t[k] + total

    pending = {}

    def opening(key, axis, far, minus, plus, into_a, into_b):
        marks = pending[key] = [copies.landing() for _ in range(3)]
        copies.send(far[0], into_a.at[0], near(axis, 1), marks[0])
        copies.send(far[1], into_a.at[1], near(axis, 3), marks[1])
        copies.send(plus[1], into_b.at[0, 1], near(axis, 1), marks[2])
        copies.send(minus[0], into_b.at[1, 0], near(axis, 3), marks[2])

    def one_start(k, a):
        far, plus, minus = ((grad.at[k, a, b, top], grad.at[k, a, b, bottom]) for b in (2, 1, 3))
        opening(("one", k, a), axes[k][0], far, minus, plus, one_a.at[k, a], one_b.at[k, a])

    def one_forward(k, a):
        axis, marks = axes[k][0], pending["one", k, a]
        copies.wait(marks[0], one_a.at[k, a, 0])
        grad[k, a, 1, 0:128] = grad[k, a, 1, 0:128] + one_a[k, a, 0]
        copies.send(grad.at[k, a, 1, top], one_b.at[k, a, 0, 0], near(axis, 1), marks[2])
        copies.wait(marks[1], one_a.at[k, a, 1])
        grad[k, a, 3, 128:256] = grad[k, a, 3, 128:256] + one_a[k, a, 1]
        copies.send(grad.at[k, a, 3, bottom], one_b.at[k, a, 1, 1], near(axis, 3), marks[2])

    def one_finish(k, a):
        copies.wait(pending["one", k, a][2], one_b.at[k, a])
        grad[k, a, 0, 0:128] = grad[k, a, 0, 0:128] + (one_b[k, a, 0, 0] + one_b[k, a, 1, 0])
        grad[k, a, 0, 128:256] = grad[k, a, 0, 128:256] + (one_b[k, a, 0, 1] + one_b[k, a, 1, 1])

    def two_start(k):
        axis = axes[k][1]
        marks = pending["two", k] = [copies.landing() for _ in range(3)]
        copies.send(grad.at[k, 2, 0, top], two_a.at[k, 0], near(axis, 1), marks[0])
        copies.send(grad.at[k, 2, 0, bottom], two_a.at[k, 1], near(axis, 3), marks[1])

    def two_plus(k):
        axis, marks = axes[k][1], pending["two", k]
        copies.send(grad.at[k, 1, 0, bottom], two_b.at[k, 0, 1], near(axis, 1), marks[2])
        copies.wait(marks[0], two_a.at[k, 0])
        grad[k, 1, 0, 0:128] = grad[k, 1, 0, 0:128] + two_a[k, 0]
        copies.send(grad.at[k, 1, 0, top], two_b.at[k, 0, 0], near(axis, 1), marks[2])

    def two_minus(k):
        axis, marks = axes[k][1], pending["two", k]
        copies.send(grad.at[k, 3, 0, top], two_b.at[k, 1, 0], near(axis, 3), marks[2])
        copies.wait(marks[1], two_a.at[k, 1])
        grad[k, 3, 0, 128:256] = grad[k, 3, 0, 128:256] + two_a[k, 1]
        copies.send(grad.at[k, 3, 0, bottom], two_b.at[k, 1, 1], near(axis, 3), marks[2])

    def two_finish(k):
        copies.wait(pending["two", k][2], two_b.at[k])
        top_sum = grad[k, 0, 0, 0:128] + (two_b[k, 0, 0] + two_b[k, 1, 0])
        bottom_sum = grad[k, 0, 0, 128:256] + (two_b[k, 0, 1] + two_b[k, 1, 1])
        return jnp.concatenate([top_sum, bottom_sum], axis=0)

    def low_rows(k, b, half=None):
        start = lax.rem(coord[axes[k][0]] + b, 4) * 64
        if half is None:
            return pl.ds(pl.multiple_of(start, 64), 64)
        return pl.ds(pl.multiple_of(start + 32 * half, 32), 32)

    def low_piece(k, a):
        first, second = axes[k]
        return pl.ds(pl.multiple_of(coord[first] * 64 + lax.rem(coord[second] + a, 4) * 16, 16), 16)

    def low_start(k):
        far, plus, minus = ([low_t.at[k, low_rows(k, b, half)] for half in range(2)] for b in (2, 1, 3))
        opening(("low", k), axes[k][0], far, minus, plus, low_a.at[k], low_b.at[k])

    def low_forward(k):
        axis, marks = axes[k][0], pending["low", k]
        copies.wait(marks[0], low_a.at[k, 0])
        rows = low_rows(k, 1, 0)
        low_t[k, rows] = low_t[k, rows] + low_a[k, 0]
        copies.send(low_t.at[k, rows], low_b.at[k, 0, 0], near(axis, 1), marks[2])
        copies.wait(marks[1], low_a.at[k, 1])
        rows = low_rows(k, 3, 1)
        low_t[k, rows] = low_t[k, rows] + low_a[k, 1]
        copies.send(low_t.at[k, rows], low_b.at[k, 1, 1], near(axis, 3), marks[2])

    def low_second(k):
        copies.wait(pending["low", k][2], low_b.at[k])
        for half in range(2):
            rows = low_rows(k, 0, half)
            low_t[k, rows] = low_t[k, rows] + (low_b[k, 0, half] + low_b[k, 1, half])
        mark = pending["low2", k] = copies.landing()
        for a in (2, 1, 3):
            copies.send(low_t.at[k, low_piece(k, a)], low_in.at[k, 3 - a], near(axes[k][1], a), mark)

    def low_third(k):
        copies.wait(pending["low2", k], low_in.at[k])
        rows = low_piece(k, 0)
        low_all[k, rows] = low_t[k, rows] + low_in[k, 0] + low_in[k, 1] + low_in[k, 2]
        mark = pending["low3", k] = copies.landing()
        for peer in fs_peers:
            copies.send(low_all.at[k, rows], low_all.at[k, rows], peer, mark)

    def moments(k):
        copies.wait(pending["low3", k], low_all.at[k, pl.ds(0, 240)])
        low = low_all[k].T
        first = 0.9 * mom1[k] + 0.1 * low
        second = 0.95 * mom2[k] + 0.05 * low * low
        out_1[k] = first
        out_2[k] = second
        normed = first / (jnp.sqrt(second) + 1e-06)
        tp_own[k] = folded(normed * normed)
        tp_own[2 + k] = folded(low * low)
        mine = fact[k, 0, 0:128, :]
        own_p[k] = sum(jnp.dot(mine, part, preferred_element_type=F32) for part in halves(normed, 3))
        own_f[k] = sum(jnp.dot(mine, part, preferred_element_type=F32) for part in halves(low, 3))

    both = range(2)
    c0, c1, c2, c3 = ORDER
    for k in both:
        transpose_right(k)
        local_grad(k, c0)
        if k == 0:
            pl.semaphore_wait(barrier, len(fs_peers) + len(tp_peers))
        one_start(k, c0)
    for k in both:
        local_grad(k, c1)
    for k in both:
        fact_in[k].wait()
        local_low(k, c0)
        one_forward(k, c0)
        one_start(k, c1)
    for k in both:
        local_low(k, c1)
    for k in both:
        local_grad(k, c2)
        local_low(k, c2)
        one_forward(k, c1)
    for k in both:
        local_grad(k, c3)
        local_low(k, c3)
        low_start(k)
        one_start(k, c2)
    for k in both:
        one_finish(k, c0)
        two_start(k)
    for k in both:
        low_forward(k)
        one_start(k, c3)
    for k in both:
        one_forward(k, c2)
    for k in both:
        low_second(k)
    for k in both:
        one_finish(k, c1)
        two_plus(k)
    for k in both:
        one_forward(k, c3)
    for k in both:
        low_third(k)
    for k in both:
        one_finish(k, c2)
        two_minus(k)
    for k in both:
        one_finish(k, c3)
    mom1_in.wait()
    mom2_in.wait()
    wts_in.wait()
    for k in both:
        moments(k)
    tp_mark, tot_mark = copies.landing(), copies.landing()
    for i, peer in enumerate(tp_peers):
        copies.send(tp_own, tp_in.at[i], peer, tp_mark)
    lane = lax.broadcasted_iota(jnp.int32, (1, 128), 1)
    row = jnp.zeros((1, 128), F32)
    for k in both:
        resid = two_finish(k).T - own_f[k]
        own_f[k] = resid
        parts = (own_p[k] * own_p[k], own_p[k] * resid, resid * resid)
        for i, part in enumerate(parts):
            row = jnp.where(lane == 3 * k + i, jnp.sum(folded(part), keepdims=True), row)
    tot_own[0:1, :] = row
    tot_in[127:128, :] = row
    for i, peer in enumerate(all_peers):
        copies.send(tot_own.at[pl.ds(0, 1)], tot_in.at[pl.ds(i, 1)], peer, tot_mark, SENDS - 1)
    copies.wait(tp_mark, tp_in)
    sums = tp_own[...]
    for i in range(len(tp_peers)):
        sums = sums + tp_in[i]
    factor = jnp.zeros((1, 128), F32)
    for k in both:
        ratio = jnp.sqrt(jnp.sum(sums[k], keepdims=True)) / jnp.sqrt(jnp.sum(sums[2 + k], keepdims=True) + 1e-06)
        out_u[k] = own_p[k] + ratio * own_f[k]
        for i, value in enumerate((jnp.ones((1, 1), F32), 2.0 * ratio, ratio * ratio)):
            factor = jnp.where(lane == 3 * k + i, value, factor)
    copies.wait(tot_mark, tot_in.at[pl.ds(0, 127)])
    total = jnp.sum(folded(tot_in[...]).sum(axis=0, keepdims=True) * factor, keepdims=True)
    scale = lax.rsqrt(total / (2.0 * 2048 * 2048) + 1e-06)

    for k in range(2):
        value = out_u[k] * scale
        out_u[k] = value
        value = wts[k] - 0.02 * value
        out_w[k] = value
        gathered[k, 0, 0] = value.astype(BF16)

    upper, lower = pl.ds(0, 64), pl.ds(64, 64)

    def spread(k, b):
        marks = pending["w", k, b] = [copies.landing() for _ in range(3)]
        copies.send(gathered.at[k, 0, b], gathered.at[k, 3, b], near(axes[k][1], 1), marks[0])
        copies.send(gathered.at[k, 0, b], gathered.at[k, 1, b], near(axes[k][1], 3), marks[1])

    def relay(k, b):
        marks = pending["w", k, b]
        copies.wait(marks[0], gathered.at[k, 3, b])
        copies.send(gathered.at[k, 3, b, upper], gathered.at[k, 2, b, upper], near(axes[k][1], 1), marks[2])
        copies.wait(marks[1], gathered.at[k, 1, b])
        copies.send(gathered.at[k, 1, b, lower], gathered.at[k, 2, b, lower], near(axes[k][1], 3), marks[2])

    def land(k, b):
        copies.wait(pending["w", k, b][2], gathered.at[k, 2, b])

    def v_start(k):
        marks = pending["v", k] = [copies.landing() for _ in range(3)]
        copies.send(gathered.at[k, 0, 0], gathered.at[k, 0, 3], near(axes[k][0], 1), marks[0])
        copies.send(gathered.at[k, 0, 0], gathered.at[k, 0, 1], near(axes[k][0], 3), marks[1])

    def v_forward(k):
        marks = pending["v", k]
        copies.wait(marks[0], gathered.at[k, 0, 3])
        copies.send(gathered.at[k, 0, 3, upper], gathered.at[k, 0, 2, upper], near(axes[k][0], 1), marks[2])
        copies.wait(marks[1], gathered.at[k, 0, 1])
        copies.send(gathered.at[k, 0, 1, lower], gathered.at[k, 0, 2, lower], near(axes[k][0], 3), marks[2])

    def v_finish(k):
        copies.wait(pending["v", k][2], gathered.at[k, 0, 2])

    for k in both:
        v_start(k)
    for k in both:
        spread(k, 0)
    for k in both:
        v_forward(k)
        spread(k, 3)
        spread(k, 1)
    for k in both:
        relay(k, 0)
    for k in both:
        v_finish(k)
        spread(k, 2)
    for b in (3, 1, 2):
        for k in both:
            relay(k, b)
    for b in (0, 3, 1, 2):
        for k in both:
            land(k, b)
    copies.wait_sent()
    pltpu.make_async_copy(tot_in.at[pl.ds(0, 127)], tot_in.at[pl.ds(0, 127)], send_sems.at[SENDS - 1]).wait()


def write_out(
    out_w, out_u, out_1, out_2, gathered, new_weights, update, new_first, new_second, weight_copy, sems
):
    z, x = lax.axis_index(Z), lax.axis_index(X)
    pairs = []
    for a in range(4):
        for b in range(4):
            for k in range(2):
                dz, dx = (a, b) if k == 0 else (b, a)
                block = lax.rem(z + dz, 4) * 4 + lax.rem(x + dx, 4)
                rows = pl.ds(pl.multiple_of(block * 128, 128), 128)
                pairs.append((gathered.at[k, a, b], weight_copy.at[k, rows, :]))
    for src, dst in pairs:
        pltpu.make_async_copy(src, dst, sems.at[0]).start()
    pairs = ((out_1, new_first), (out_2, new_second), (out_w, new_weights), (out_u, update))
    copies = [pltpu.make_async_copy(*pair, sems.at[1 + i]) for i, pair in enumerate(pairs)]
    for copy in copies:
        copy.start()
    for copy in copies:
        copy.wait()
    pltpu.make_async_copy(gathered, gathered, sems.at[0]).wait()


def per_device(*args):
    any_space = pl.BlockSpec(memory_space=pl.ANY)
    vmem_space = pl.BlockSpec(memory_space=pltpu.VMEM)
    held = (
        ((2, 128, 256), F32),
        ((2, 128, 256), F32),
        ((2, 256, 256), F32),
        ((2, 256, 256), F32),
        ((2, 4, 4, 128, 256), BF16),
    )
    dma = pltpu.SemaphoreType.DMA
    results = pl.pallas_call(
        kernel,
        name="step",
        out_shape=[pltpu.VMEM(*shape) for shape in held],
        in_specs=[any_space] * 8,
        out_specs=[vmem_space] * 5,
        scratch_shapes=[
            pltpu.VMEM((2, 4, 2560, 512), BF16),
            pltpu.VMEM((2, 2560, 256), BF16),
            pltpu.VMEM((2, 256, 2560), BF16),
            pltpu.VMEM((2, 4, 512, 256), BF16),
            pltpu.VMEM((2, 4, 4, 256, 128), F32),
            pltpu.VMEM((2, 4, 2, 128, 128), F32),
            pltpu.VMEM((2, 4, 2, 2, 128, 128), F32),
            pltpu.VMEM((2, 2, 128, 128), F32),
            pltpu.VMEM((2, 2, 2, 128, 128), F32),
            pltpu.VMEM((2, 256, 256), F32),
            pltpu.VMEM((2, 2, 32, 256), F32),
            pltpu.VMEM((2, 2, 2, 32, 256), F32),
            pltpu.VMEM((2, 3, 16, 256), F32),
            pltpu.VMEM((2, 256, 256), F32),
            pltpu.VMEM((2, 128, 256), F32),
            pltpu.VMEM((2, 256, 256), F32),
            pltpu.VMEM((2, 256, 256), F32),
            pltpu.VMEM((2, 128, 256), F32),
            pltpu.VMEM((2, 128, 256), F32),
            pltpu.VMEM((4, 8, 128), F32),
            pltpu.VMEM((7, 4, 8, 128), F32),
            pltpu.VMEM((8, 128), F32),
            pltpu.VMEM((128, 128), F32),
            dma((LOADS,)),
            dma((SENDS,)),
            dma((LANDINGS,)),
        ],
        compiler_params=pltpu.CompilerParams(
            collective_id=0, has_side_effects=True, vmem_limit_bytes=60 * 1024 * 1024
        ),
    )(*args)
    return pl.pallas_call(
        write_out,
        name="write_out",
        out_shape=[jax.ShapeDtypeStruct(shape, kind) for shape, kind in held[:4]]
        + [jax.ShapeDtypeStruct((2, 2048, 256), BF16)],
        in_specs=[vmem_space] * 5,
        out_specs=[any_space] * 5,
        scratch_shapes=[dma((5,))],
        compiler_params=pltpu.CompilerParams(vmem_limit_bytes=1024 * 1024),
    )(*results)


def solution(mesh):
    finer = Mesh(mesh.devices.reshape(4, 4, 4, 2), (Z, X, Y, C))
    in_specs = (
        P(FS, None),
        P(FS, None),
        P(FS, TP),
        P(FS, TP),
        P(None, FS, TP),
        P(),
        P(None, None, TP),
        P(None, None, TP),
    )
    out_specs = (
        P(None, FS, TP),
        P(None, FS, TP),
        P(None, None, TP),
        P(None, None, TP),
        P(None, None, TP),
    )
    return jax.shard_map(per_device, mesh=finer, in_specs=in_specs, out_specs=out_specs, check_vma=False)
```

```python
import math

import jax
import jax.numpy as jnp
from jax import lax
from jax.experimental import pallas as pl
from jax.experimental.pallas import tpu as pltpu
from jax.sharding import Mesh
from jax.sharding import PartitionSpec as P

Z, X, Y, C = "fs_0", "fs_1", "tp_0", "tp_1"
FS, TP = (Z, X), (Y, C)
MESH = pl.DeviceIdType.MESH
F32, BF16 = jnp.float32, jnp.bfloat16
ORDER = (2, 1, 3, 0)


class Copies:
    def __init__(self, send_sems, recv_sems, spare):
        self.send_sems, self.recv_sems, self.spare = send_sems, recv_sems, spare
        self.landings, self.sent = 0, [0]

    def landing(self):
        self.landings += 1
        return self.landings - 1

    def send(self, src, dst, device, landing, own=None):
        size = math.prod(src.shape) * src.dtype.itemsize // 1024
        if own is None:
            if self.sent[-1] + size > self.spare.shape[0]:
                self.sent.append(0)
            self.sent[-1] += size
        pltpu.make_async_remote_copy(
            src_ref=src,
            dst_ref=dst,
            send_sem=self.send_sems.at[len(self.sent) - 1 if own is None else own],
            recv_sem=self.recv_sems.at[landing],
            device_id=device,
            device_id_type=MESH,
        ).start()

    def wait(self, landing, place):
        pltpu.make_async_copy(place, place, self.recv_sems.at[landing]).wait()

    def wait_sent(self):
        for index, size in enumerate(self.sent):
            rows = self.spare.at[pl.ds(0, size)]
            pltpu.make_async_copy(rows, rows, self.send_sems.at[index]).wait()


SENDS, LANDINGS, LOADS = 4, 77, 15


def halves(value, terms):
    out = []
    for _ in range(terms - 1):
        part = value.astype(BF16)
        out.append(part)
        value = value - part.astype(F32)
    out.append(value.astype(BF16))
    return out


def folded(value):
    rows, cols = value.shape
    total = value[:, 0:128]
    for start in range(128, cols, 128):
        total = total + value[:, start : start + 128]
    return total.reshape(rows // 8, 8, 128).sum(axis=0)


def kernel(
    layer_inputs, output_cot, query_cot, head_outputs, weights, factors, first_moment, second_moment,
    out_w, out_u, out_1, out_2, gathered,
    left, right, right_t, fact, grad, one_a, one_b, two_a, two_b,
    low_t, low_a, low_b, low_in, low_all, wts, mom1, mom2,
    own_p, own_f, own_g, grams, mom1_t, mom2_t, tot_own, tot_in,
    load_sems, send_sems, recv_sems,
):
    z, x, y, c = (lax.axis_index(name) for name in (Z, X, Y, C))
    lefts, rights = (layer_inputs, output_cot), (query_cot, head_outputs)
    coord = {Z: z, X: x, Y: y, C: c}
    axes = ((X, Z), (Z, X))

    def near(axis, delta):
        return {axis: lax.rem(coord[axis] + delta, 4)}

    def place(k, a, b):
        first, second = axes[k]
        at = {first: lax.rem(coord[first] + b, 4), second: lax.rem(coord[second] + a, 4)}
        return at[Z] * 4 + at[X]

    loads = []

    def load(pairs, whole):
        sem = load_sems.at[len(loads)]
        for src, dst in pairs:
            pltpu.make_async_copy(src, dst, sem).start()
        loads.append(pltpu.make_async_copy(whole, whole, sem))
        return loads[-1]

    def load_left(k, a):
        pairs = []
        for b in range(4):
            cols = pl.ds(pl.multiple_of(place(k, a, b) * 128, 128), 128)
            pairs.append((lefts[k].at[:, cols], left.at[k, a, :, pl.ds(128 * b, 128)]))
        return load(pairs, left.at[k, a])

    def load_factors(k):
        pairs = []
        for a in range(4):
            for b in range(4):
                rows = pl.ds(pl.multiple_of(place(k, a, b) * 128, 128), 128)
                pairs.append((factors.at[k, rows, :], fact.at[k, a, pl.ds(128 * b, 128), :]))
        return load(pairs, fact.at[k])

    right_in, left_in, fact_in = [None] * 2, {}, [None] * 2
    for k in range(2):
        right_in[k] = load([(rights[k], right.at[k])], right.at[k])
        left_in[k, ORDER[0]] = load_left(k, ORDER[0])
    for k in range(2):
        left_in[k, ORDER[1]] = load_left(k, ORDER[1])
    for k in range(2):
        fact_in[k] = load_factors(k)
    for a in ORDER[2:]:
        for k in range(2):
            left_in[k, a] = load_left(k, a)
    mom1_in = load([(first_moment, mom1)], mom1)
    mom2_in = load([(second_moment, mom2)], mom2)
    wts_in = load([(weights, wts)], wts)

    barrier = pltpu.get_barrier_semaphore()
    fs_peers = [
        {Z: lax.rem(z + dz, 4), X: lax.rem(x + dx, 4)} for dz in range(4) for dx in range(4) if dz or dx
    ]
    tp_peers = [
        {Y: lax.rem(y + dy, 4), C: lax.rem(c + dc, 2)} for dy in range(4) for dc in range(2) if dy or dc
    ]
    all_peers = [
        {Z: lax.rem(z + dz, 4), X: lax.rem(x + dx, 4), Y: lax.rem(y + dy, 4), C: lax.rem(c + dc, 2)}
        for dz in ORDER
        for dx in ORDER
        for dy in ORDER
        for dc in range(2)
        if dz or dx or dy or dc
    ]
    for peer in fs_peers + tp_peers:
        pl.semaphore_signal(barrier, inc=1, device_id=peer, device_id_type=MESH)

    copies = Copies(send_sems, recv_sems, left.at[0, 0])
    top, bottom = pl.ds(0, 128), pl.ds(128, 128)

    def transpose_right(k):
        right_in[k].wait()
        for start in range(0, 2560, 256):
            right_t[k, :, start : start + 256] = right[k, start : start + 256, :].T

    def local_grad(k, a):
        left_in[k, a].wait()
        value = jnp.dot(right_t[k], left[k, a], preferred_element_type=F32)
        for b in range(4):
            grad[k, a, b] = value[:, 128 * b : 128 * b + 128]

    def local_low(k, a):
        total = None
        value = jnp.concatenate([grad[k, a, b] for b in range(4)], axis=1)
        for part in halves(value, 2):
            term = jnp.dot(part, fact[k, a], preferred_element_type=F32)
            total = term if total is None else total + term
        if a == ORDER[0]:
            low_t[k] = total
        else:
            low_t[k] = low_t[k] + total

    pending = {}

    def opening(key, axis, far, minus, plus, into_a, into_b):
        marks = pending[key] = [copies.landing() for _ in range(3)]
        copies.send(far[0], into_a.at[0], near(axis, 1), marks[0])
        copies.send(far[1], into_a.at[1], near(axis, 3), marks[1])
        copies.send(plus[1], into_b.at[0, 1], near(axis, 1), marks[2])
        copies.send(minus[0], into_b.at[1, 0], near(axis, 3), marks[2])

    def one_start(k, a):
        far, plus, minus = ((grad.at[k, a, b, top], grad.at[k, a, b, bottom]) for b in (2, 1, 3))
        opening(("one", k, a), axes[k][0], far, minus, plus, one_a.at[k, a], one_b.at[k, a])

    def one_forward(k, a):
        axis, marks = axes[k][0], pending["one", k, a]
        copies.wait(marks[0], one_a.at[k, a, 0])
        grad[k, a, 1, 0:128] = grad[k, a, 1, 0:128] + one_a[k, a, 0]
        copies.send(grad.at[k, a, 1, top], one_b.at[k, a, 0, 0], near(axis, 1), marks[2])
        copies.wait(marks[1], one_a.at[k, a, 1])
        grad[k, a, 3, 128:256] = grad[k, a, 3, 128:256] + one_a[k, a, 1]
        copies.send(grad.at[k, a, 3, bottom], one_b.at[k, a, 1, 1], near(axis, 3), marks[2])

    def one_finish(k, a):
        copies.wait(pending["one", k, a][2], one_b.at[k, a])
        grad[k, a, 0, 0:128] = grad[k, a, 0, 0:128] + (one_b[k, a, 0, 0] + one_b[k, a, 1, 0])
        grad[k, a, 0, 128:256] = grad[k, a, 0, 128:256] + (one_b[k, a, 0, 1] + one_b[k, a, 1, 1])

    def two_start(k):
        axis = axes[k][1]
        marks = pending["two", k] = [copies.landing() for _ in range(3)]
        copies.send(grad.at[k, 2, 0, top], two_a.at[k, 0], near(axis, 1), marks[0])
        copies.send(grad.at[k, 2, 0, bottom], two_a.at[k, 1], near(axis, 3), marks[1])

    def two_plus(k):
        axis, marks = axes[k][1], pending["two", k]
        copies.send(grad.at[k, 1, 0, bottom], two_b.at[k, 0, 1], near(axis, 1), marks[2])
        copies.wait(marks[0], two_a.at[k, 0])
        grad[k, 1, 0, 0:128] = grad[k, 1, 0, 0:128] + two_a[k, 0]
        copies.send(grad.at[k, 1, 0, top], two_b.at[k, 0, 0], near(axis, 1), marks[2])

    def two_minus(k):
        axis, marks = axes[k][1], pending["two", k]
        copies.send(grad.at[k, 3, 0, top], two_b.at[k, 1, 0], near(axis, 3), marks[2])
        copies.wait(marks[1], two_a.at[k, 1])
        grad[k, 3, 0, 128:256] = grad[k, 3, 0, 128:256] + two_a[k, 1]
        copies.send(grad.at[k, 3, 0, bottom], two_b.at[k, 1, 1], near(axis, 3), marks[2])

    def two_finish(k):
        copies.wait(pending["two", k][2], two_b.at[k])
        top_sum = grad[k, 0, 0, 0:128] + (two_b[k, 0, 0] + two_b[k, 1, 0])
        bottom_sum = grad[k, 0, 0, 128:256] + (two_b[k, 0, 1] + two_b[k, 1, 1])
        return jnp.concatenate([top_sum, bottom_sum], axis=0)

    def low_rows(k, b, half=None):
        start = lax.rem(coord[axes[k][0]] + b, 4) * 64
        if half is None:
            return pl.ds(pl.multiple_of(start, 64), 64)
        return pl.ds(pl.multiple_of(start + 32 * half, 32), 32)

    def low_piece(k, a):
        first, second = axes[k]
        return pl.ds(pl.multiple_of(coord[first] * 64 + lax.rem(coord[second] + a, 4) * 16, 16), 16)

    def low_start(k):
        far, plus, minus = ([low_t.at[k, low_rows(k, b, half)] for half in range(2)] for b in (2, 1, 3))
        opening(("low", k), axes[k][0], far, minus, plus, low_a.at[k], low_b.at[k])

    def low_forward(k):
        axis, marks = axes[k][0], pending["low", k]
        copies.wait(marks[0], low_a.at[k, 0])
        rows = low_rows(k, 1, 0)
        low_t[k, rows] = low_t[k, rows] + low_a[k, 0]
        copies.send(low_t.at[k, rows], low_b.at[k, 0, 0], near(axis, 1), marks[2])
        copies.wait(marks[1], low_a.at[k, 1])
        rows = low_rows(k, 3, 1)
        low_t[k, rows] = low_t[k, rows] + low_a[k, 1]
        copies.send(low_t.at[k, rows], low_b.at[k, 1, 1], near(axis, 3), marks[2])

    def low_second(k):
        copies.wait(pending["low", k][2], low_b.at[k])
        for half in range(2):
            rows = low_rows(k, 0, half)
            low_t[k, rows] = low_t[k, rows] + (low_b[k, 0, half] + low_b[k, 1, half])
        mark = pending["low2", k] = copies.landing()
        for a in (2, 1, 3):
            copies.send(low_t.at[k, low_piece(k, a)], low_in.at[k, 3 - a], near(axes[k][1], a), mark)

    def low_third(k):
        copies.wait(pending["low2", k], low_in.at[k])
        rows = low_piece(k, 0)
        low_all[k, rows] = low_t[k, rows] + low_in[k, 0] + low_in[k, 1] + low_in[k, 2]
        mark = pending["low3", k] = copies.landing()
        for a in (2, 1, 3):
            copies.send(low_all.at[k, rows], low_all.at[k, rows], near(axes[k][1], a), mark)

    def low_fourth(k):
        copies.wait(pending["low3", k], low_all.at[k, pl.ds(0, 48)])
        axis, rows = axes[k][0], low_rows(k, 0)
        marks = pending["low4", k] = [copies.landing() for _ in range(3)]
        copies.send(low_all.at[k, rows], low_all.at[k, rows], near(axis, 1), marks[0])
        copies.send(low_all.at[k, rows], low_all.at[k, rows], near(axis, 3), marks[1])

    def low_fifth(k):
        axis, marks = axes[k][0], pending["low4", k]
        copies.wait(marks[0], low_all.at[k, pl.ds(0, 64)])
        rows = low_rows(k, 3, 0)
        copies.send(low_all.at[k, rows], low_all.at[k, rows], near(axis, 1), marks[2])
        copies.wait(marks[1], low_all.at[k, pl.ds(0, 64)])
        rows = low_rows(k, 1, 1)
        copies.send(low_all.at[k, rows], low_all.at[k, rows], near(axis, 3), marks[2])

    def gram(k):
        total = None
        for a in range(4):
            rows = fact[k, a]
            term = jnp.dot(rows.T, rows, preferred_element_type=F32)
            total = term if total is None else total + term
        for i, part in enumerate(halves(total, 2)):
            grams[k, i] = part

    def turn(k):
        mom1_t[k] = mom1[k].T
        mom2_t[k] = mom2[k].T

    def own_terms(k):
        rows = low_piece(k, 0)
        low = low_all[k, rows, :]
        first = 0.9 * mom1_t[k, rows, :] + 0.1 * low
        second = 0.95 * mom2_t[k, rows, :] + 0.05 * low * low
        normed = first / (jnp.sqrt(second) + 1e-06)
        stack = jnp.concatenate(halves(normed, 2) + halves(low, 2), axis=0)
        product = sum(jnp.dot(stack, grams[k, i], preferred_element_type=F32) for i in range(2))
        by_normed = product[0:16] + product[16:32]
        by_low = product[32:48] + product[48:64]
        pairs = ((normed, by_normed), (normed, low), (normed, by_low), (low, low), (low, by_low), (normed, normed))
        row = jnp.zeros((1, 128), F32)
        for i, (one, other) in enumerate(pairs):
            row = jnp.where(lane == 8 * k + i, jnp.sum(folded(one * other), keepdims=True), row)
        return row

    def moments(k):
        copies.wait(pending["low4", k][2], low_all.at[k, pl.ds(0, 64)])
        low = low_all[k].T
        first = 0.9 * mom1[k] + 0.1 * low
        second = 0.95 * mom2[k] + 0.05 * low * low
        out_1[k] = first
        out_2[k] = second
        normed = first / (jnp.sqrt(second) + 1e-06)
        mine = fact[k, 0, 0:128, :]
        own_p[k] = sum(jnp.dot(mine, part, preferred_element_type=F32) for part in halves(normed, 3))
        own_f[k] = own_g[k].T - sum(jnp.dot(mine, part, preferred_element_type=F32) for part in halves(low, 3))

    lane = lax.broadcasted_iota(jnp.int32, (1, 128), 1)
    both = range(2)
    c0, c1, c2, c3 = ORDER
    for k in both:
        transpose_right(k)
        local_grad(k, c0)
        if k == 0:
            pl.semaphore_wait(barrier, len(fs_peers) + len(tp_peers))
        one_start(k, c0)
    for k in both:
        local_grad(k, c1)
    for k in both:
        fact_in[k].wait()
        local_low(k, c0)
        one_forward(k, c0)
        one_start(k, c1)
    for k in both:
        local_low(k, c1)
    for k in both:
        local_grad(k, c2)
        local_low(k, c2)
        one_forward(k, c1)
    for k in both:
        local_grad(k, c3)
        local_low(k, c3)
        low_start(k)
        one_start(k, c2)
    for k in both:
        one_finish(k, c0)
        two_start(k)
    for k in both:
        gram(k)
    for k in both:
        low_forward(k)
        one_start(k, c3)
    for k in both:
        one_forward(k, c2)
    mom1_in.wait()
    mom2_in.wait()
    wts_in.wait()
    for k in both:
        turn(k)
    for k in both:
        low_second(k)
    for k in both:
        one_finish(k, c1)
        two_plus(k)
    for k in both:
        one_forward(k, c3)
    for k in both:
        low_third(k)
    for k in both:
        one_finish(k, c2)
        two_minus(k)
    row = own_terms(0) + own_terms(1)
    for k in both:
        one_finish(k, c3)
    for k in both:
        own = two_finish(k)
        own_g[k] = own
        row = jnp.where(lane == 8 * k + 6, jnp.sum(folded(own * own), keepdims=True), row)
    tot_own[0:1, :] = row
    tot_in[127:128, :] = row
    tot_mark = copies.landing()
    for i, peer in enumerate(all_peers):
        copies.send(tot_own.at[pl.ds(0, 1)], tot_in.at[pl.ds(i, 1)], peer, tot_mark, SENDS - 1)
    for k in both:
        low_fourth(k)
    for k in both:
        low_fifth(k)
    for k in both:
        moments(k)
    copies.wait(tot_mark, tot_in.at[pl.ds(0, 127)])
    sums = folded(tot_in[...]).sum(axis=0, keepdims=True)
    total, ratios = None, []
    for k in both:
        part = [jnp.sum(jnp.where(lane == 8 * k + i, sums, 0.0), keepdims=True) for i in range(7)]
        ratio = jnp.sqrt(part[5]) / jnp.sqrt(part[3] + 1e-06)
        value = part[0] + 2.0 * ratio * (part[1] - part[2]) + ratio * ratio * (part[6] - 2.0 * part[3] + part[4])
        total = value if total is None else total + value
        ratios.append(ratio)
    scale = lax.rsqrt(jnp.maximum(total, 0.0) / (2.0 * 2048 * 2048) + 1e-06)

    for k in range(2):
        value = (own_p[k] + ratios[k] * own_f[k]) * scale
        out_u[k] = value
        value = wts[k] - 0.02 * value
        out_w[k] = value
        gathered[k, 0, 0] = value.astype(BF16)

    upper, lower = pl.ds(0, 64), pl.ds(64, 64)

    def spread(k, b):
        marks = pending["w", k, b] = [copies.landing() for _ in range(3)]
        copies.send(gathered.at[k, 0, b], gathered.at[k, 3, b], near(axes[k][1], 1), marks[0])
        copies.send(gathered.at[k, 0, b], gathered.at[k, 1, b], near(axes[k][1], 3), marks[1])

    def relay(k, b):
        marks = pending["w", k, b]
        copies.wait(marks[0], gathered.at[k, 3, b])
        copies.send(gathered.at[k, 3, b, upper], gathered.at[k, 2, b, upper], near(axes[k][1], 1), marks[2])
        copies.wait(marks[1], gathered.at[k, 1, b])
        copies.send(gathered.at[k, 1, b, lower], gathered.at[k, 2, b, lower], near(axes[k][1], 3), marks[2])

    def land(k, b):
        copies.wait(pending["w", k, b][2], gathered.at[k, 2, b])

    def v_start(k):
        marks = pending["v", k] = [copies.landing() for _ in range(3)]
        copies.send(gathered.at[k, 0, 0], gathered.at[k, 0, 3], near(axes[k][0], 1), marks[0])
        copies.send(gathered.at[k, 0, 0], gathered.at[k, 0, 1], near(axes[k][0], 3), marks[1])

    def v_forward(k):
        marks = pending["v", k]
        copies.wait(marks[0], gathered.at[k, 0, 3])
        copies.send(gathered.at[k, 0, 3, upper], gathered.at[k, 0, 2, upper], near(axes[k][0], 1), marks[2])
        copies.wait(marks[1], gathered.at[k, 0, 1])
        copies.send(gathered.at[k, 0, 1, lower], gathered.at[k, 0, 2, lower], near(axes[k][0], 3), marks[2])

    def v_finish(k):
        copies.wait(pending["v", k][2], gathered.at[k, 0, 2])

    for k in both:
        v_start(k)
    for k in both:
        spread(k, 0)
    for k in both:
        v_forward(k)
        spread(k, 3)
        spread(k, 1)
    for k in both:
        relay(k, 0)
    for k in both:
        v_finish(k)
        spread(k, 2)
    for b in (3, 1, 2):
        for k in both:
            relay(k, b)
    for b in (0, 3, 1, 2):
        for k in both:
            land(k, b)
    copies.wait_sent()
    pltpu.make_async_copy(tot_in.at[pl.ds(0, 127)], tot_in.at[pl.ds(0, 127)], send_sems.at[SENDS - 1]).wait()


def write_out(
    out_w, out_u, out_1, out_2, gathered, new_weights, update, new_first, new_second, weight_copy, sems
):
    z, x = lax.axis_index(Z), lax.axis_index(X)
    pairs = []
    for a in range(4):
        for b in range(4):
            for k in range(2):
                dz, dx = (a, b) if k == 0 else (b, a)
                block = lax.rem(z + dz, 4) * 4 + lax.rem(x + dx, 4)
                rows = pl.ds(pl.multiple_of(block * 128, 128), 128)
                pairs.append((gathered.at[k, a, b], weight_copy.at[k, rows, :]))
    for src, dst in pairs:
        pltpu.make_async_copy(src, dst, sems.at[0]).start()
    pairs = ((out_1, new_first), (out_2, new_second), (out_w, new_weights), (out_u, update))
    copies = [pltpu.make_async_copy(*pair, sems.at[1 + i]) for i, pair in enumerate(pairs)]
    for copy in copies:
        copy.start()
    for copy in copies:
        copy.wait()
    pltpu.make_async_copy(gathered, gathered, sems.at[0]).wait()


def per_device(*args):
    any_space = pl.BlockSpec(memory_space=pl.ANY)
    vmem_space = pl.BlockSpec(memory_space=pltpu.VMEM)
    held = (
        ((2, 128, 256), F32),
        ((2, 128, 256), F32),
        ((2, 256, 256), F32),
        ((2, 256, 256), F32),
        ((2, 4, 4, 128, 256), BF16),
    )
    dma = pltpu.SemaphoreType.DMA
    results = pl.pallas_call(
        kernel,
        name="step",
        out_shape=[pltpu.VMEM(*shape) for shape in held],
        in_specs=[any_space] * 8,
        out_specs=[vmem_space] * 5,
        scratch_shapes=[
            pltpu.VMEM((2, 4, 2560, 512), BF16),
            pltpu.VMEM((2, 2560, 256), BF16),
            pltpu.VMEM((2, 256, 2560), BF16),
            pltpu.VMEM((2, 4, 512, 256), BF16),
            pltpu.VMEM((2, 4, 4, 256, 128), F32),
            pltpu.VMEM((2, 4, 2, 128, 128), F32),
            pltpu.VMEM((2, 4, 2, 2, 128, 128), F32),
            pltpu.VMEM((2, 2, 128, 128), F32),
            pltpu.VMEM((2, 2, 2, 128, 128), F32),
            pltpu.VMEM((2, 256, 256), F32),
            pltpu.VMEM((2, 2, 32, 256), F32),
            pltpu.VMEM((2, 2, 2, 32, 256), F32),
            pltpu.VMEM((2, 3, 16, 256), F32),
            pltpu.VMEM((2, 256, 256), F32),
            pltpu.VMEM((2, 128, 256), F32),
            pltpu.VMEM((2, 256, 256), F32),
            pltpu.VMEM((2, 256, 256), F32),
            pltpu.VMEM((2, 128, 256), F32),
            pltpu.VMEM((2, 128, 256), F32),
            pltpu.VMEM((2, 256, 128), F32),
            pltpu.VMEM((2, 2, 256, 256), BF16),
            pltpu.VMEM((2, 256, 256), F32),
            pltpu.VMEM((2, 256, 256), F32),
            pltpu.VMEM((8, 128), F32),
            pltpu.VMEM((128, 128), F32),
            dma((LOADS,)),
            dma((SENDS,)),
            dma((LANDINGS,)),
        ],
        compiler_params=pltpu.CompilerParams(
            collective_id=0, has_side_effects=True, vmem_limit_bytes=60 * 1024 * 1024
        ),
    )(*args)
    return pl.pallas_call(
        write_out,
        name="write_out",
        out_shape=[jax.ShapeDtypeStruct(shape, kind) for shape, kind in held[:4]]
        + [jax.ShapeDtypeStruct((2, 2048, 256), BF16)],
        in_specs=[vmem_space] * 5,
        out_specs=[any_space] * 5,
        scratch_shapes=[dma((5,))],
        compiler_params=pltpu.CompilerParams(vmem_limit_bytes=1024 * 1024),
    )(*results)


def solution(mesh):
    finer = Mesh(mesh.devices.reshape(4, 4, 4, 2), (Z, X, Y, C))
    in_specs = (
        P(FS, None),
        P(FS, None),
        P(FS, TP),
        P(FS, TP),
        P(None, FS, TP),
        P(),
        P(None, None, TP),
        P(None, None, TP),
    )
    out_specs = (
        P(None, FS, TP),
        P(None, FS, TP),
        P(None, None, TP),
        P(None, None, TP),
        P(None, None, TP),
    )
    return jax.shard_map(per_device, mesh=finer, in_specs=in_specs, out_specs=out_specs, check_vma=False)
```

```python
import math

import jax
import jax.numpy as jnp
from jax import lax
from jax.experimental import pallas as pl
from jax.experimental.pallas import tpu as pltpu
from jax.sharding import Mesh
from jax.sharding import PartitionSpec as P

Z, X, Y, C = "fs_0", "fs_1", "tp_0", "tp_1"
FS, TP = (Z, X), (Y, C)
MESH = pl.DeviceIdType.MESH
F32, BF16 = jnp.float32, jnp.bfloat16
ORDER = (2, 1, 3, 0)


class Copies:
    def __init__(self, send_sems, recv_sems, spare):
        self.send_sems, self.recv_sems, self.spare = send_sems, recv_sems, spare
        self.landings, self.sent = 0, [0]

    def landing(self):
        self.landings += 1
        return self.landings - 1

    def send(self, src, dst, device, landing, own=None):
        size = math.prod(src.shape) * src.dtype.itemsize // 1024
        if own is None:
            if self.sent[-1] + size > self.spare.shape[0]:
                self.sent.append(0)
            self.sent[-1] += size
        pltpu.make_async_remote_copy(
            src_ref=src,
            dst_ref=dst,
            send_sem=self.send_sems.at[len(self.sent) - 1 if own is None else own],
            recv_sem=self.recv_sems.at[landing],
            device_id=device,
            device_id_type=MESH,
        ).start()

    def wait(self, landing, place):
        pltpu.make_async_copy(place, place, self.recv_sems.at[landing]).wait()

    def wait_sent(self):
        for index, size in enumerate(self.sent):
            rows = self.spare.at[pl.ds(0, size)]
            pltpu.make_async_copy(rows, rows, self.send_sems.at[index]).wait()


SENDS, LANDINGS, LOADS = 4, 78, 15


def halves(value, terms):
    out = []
    for _ in range(terms - 1):
        part = value.astype(BF16)
        out.append(part)
        value = value - part.astype(F32)
    out.append(value.astype(BF16))
    return out


def folded(value):
    rows, cols = value.shape
    total = value[:, 0:128]
    for start in range(128, cols, 128):
        total = total + value[:, start : start + 128]
    return total.reshape(rows // 8, 8, 128).sum(axis=0)


def kernel(
    layer_inputs, output_cot, query_cot, head_outputs, weights, factors, first_moment, second_moment,
    out_w, out_u, out_1, out_2, gathered,
    left, right, right_t, fact, grad, one_a, one_b, two_a, two_b,
    low_t, low_a, low_b, low_in, low_all, wts, mom1, mom2,
    own_p, own_f, own_g, grams, mom1_t, mom2_t, pair_own, pair_in, tot_own, tot_in,
    load_sems, send_sems, recv_sems,
):
    z, x, y, c = (lax.axis_index(name) for name in (Z, X, Y, C))
    lefts, rights = (layer_inputs, output_cot), (query_cot, head_outputs)
    coord = {Z: z, X: x, Y: y, C: c}
    axes = ((X, Z), (Z, X))

    def near(axis, delta):
        return {axis: lax.rem(coord[axis] + delta, 4)}

    def place(k, a, b):
        first, second = axes[k]
        at = {first: lax.rem(coord[first] + b, 4), second: lax.rem(coord[second] + a, 4)}
        return at[Z] * 4 + at[X]

    loads = []

    def load(pairs, whole):
        sem = load_sems.at[len(loads)]
        for src, dst in pairs:
            pltpu.make_async_copy(src, dst, sem).start()
        loads.append(pltpu.make_async_copy(whole, whole, sem))
        return loads[-1]

    def load_left(k, a):
        pairs = []
        for b in range(4):
            cols = pl.ds(pl.multiple_of(place(k, a, b) * 128, 128), 128)
            pairs.append((lefts[k].at[:, cols], left.at[k, a, :, pl.ds(128 * b, 128)]))
        return load(pairs, left.at[k, a])

    def load_factors(k):
        pairs = []
        for a in range(4):
            for b in range(4):
                rows = pl.ds(pl.multiple_of(place(k, a, b) * 128, 128), 128)
                pairs.append((factors.at[k, rows, :], fact.at[k, a, pl.ds(128 * b, 128), :]))
        return load(pairs, fact.at[k])

    right_in, left_in, fact_in = [None] * 2, {}, [None] * 2
    for k in range(2):
        right_in[k] = load([(rights[k], right.at[k])], right.at[k])
        left_in[k, ORDER[0]] = load_left(k, ORDER[0])
    for k in range(2):
        left_in[k, ORDER[1]] = load_left(k, ORDER[1])
    for k in range(2):
        fact_in[k] = load_factors(k)
    for a in ORDER[2:]:
        for k in range(2):
            left_in[k, a] = load_left(k, a)
    mom1_in = load([(first_moment, mom1)], mom1)
    mom2_in = load([(second_moment, mom2)], mom2)
    wts_in = load([(weights, wts)], wts)

    barrier = pltpu.get_barrier_semaphore()
    fs_peers = [
        {Z: lax.rem(z + dz, 4), X: lax.rem(x + dx, 4)} for dz in range(4) for dx in range(4) if dz or dx
    ]
    tp_peers = [
        {Y: lax.rem(y + dy, 4), C: lax.rem(c + dc, 2)} for dy in range(4) for dc in range(2) if dy or dc
    ]
    all_peers = [
        {Z: lax.rem(z + dz, 4), X: lax.rem(x + dx, 4), Y: lax.rem(y + dy, 4)}
        for dz in ORDER
        for dx in ORDER
        for dy in ORDER
        if dz or dx or dy
    ]
    for peer in fs_peers + tp_peers:
        pl.semaphore_signal(barrier, inc=1, device_id=peer, device_id_type=MESH)

    copies = Copies(send_sems, recv_sems, left.at[0, 0])
    top, bottom = pl.ds(0, 128), pl.ds(128, 128)

    def transpose_right(k):
        right_in[k].wait()
        for start in range(0, 2560, 256):
            right_t[k, :, start : start + 256] = right[k, start : start + 256, :].T

    def local_grad(k, a):
        left_in[k, a].wait()
        value = jnp.dot(right_t[k], left[k, a], preferred_element_type=F32)
        for b in range(4):
            grad[k, a, b] = value[:, 128 * b : 128 * b + 128]

    def local_low(k, a):
        total = None
        value = jnp.concatenate([grad[k, a, b] for b in range(4)], axis=1)
        for part in halves(value, 2):
            term = jnp.dot(part, fact[k, a], preferred_element_type=F32)
            total = term if total is None else total + term
        if a == ORDER[0]:
            low_t[k] = total
        else:
            low_t[k] = low_t[k] + total

    pending = {}

    def opening(key, axis, far, minus, plus, into_a, into_b):
        marks = pending[key] = [copies.landing() for _ in range(3)]
        copies.send(far[0], into_a.at[0], near(axis, 1), marks[0])
        copies.send(far[1], into_a.at[1], near(axis, 3), marks[1])
        copies.send(plus[1], into_b.at[0, 1], near(axis, 1), marks[2])
        copies.send(minus[0], into_b.at[1, 0], near(axis, 3), marks[2])

    def one_start(k, a):
        far, plus, minus = ((grad.at[k, a, b, top], grad.at[k, a, b, bottom]) for b in (2, 1, 3))
        opening(("one", k, a), axes[k][0], far, minus, plus, one_a.at[k, a], one_b.at[k, a])

    def one_forward(k, a):
        axis, marks = axes[k][0], pending["one", k, a]
        copies.wait(marks[0], one_a.at[k, a, 0])
        grad[k, a, 1, 0:128] = grad[k, a, 1, 0:128] + one_a[k, a, 0]
        copies.send(grad.at[k, a, 1, top], one_b.at[k, a, 0, 0], near(axis, 1), marks[2])
        copies.wait(marks[1], one_a.at[k, a, 1])
        grad[k, a, 3, 128:256] = grad[k, a, 3, 128:256] + one_a[k, a, 1]
        copies.send(grad.at[k, a, 3, bottom], one_b.at[k, a, 1, 1], near(axis, 3), marks[2])

    def one_finish(k, a):
        copies.wait(pending["one", k, a][2], one_b.at[k, a])
        grad[k, a, 0, 0:128] = grad[k, a, 0, 0:128] + (one_b[k, a, 0, 0] + one_b[k, a, 1, 0])
        grad[k, a, 0, 128:256] = grad[k, a, 0, 128:256] + (one_b[k, a, 0, 1] + one_b[k, a, 1, 1])

    def two_start(k):
        axis = axes[k][1]
        marks = pending["two", k] = [copies.landing() for _ in range(3)]
        copies.send(grad.at[k, 2, 0, top], two_a.at[k, 0], near(axis, 1), marks[0])
        copies.send(grad.at[k, 2, 0, bottom], two_a.at[k, 1], near(axis, 3), marks[1])

    def two_plus(k):
        axis, marks = axes[k][1], pending["two", k]
        copies.send(grad.at[k, 1, 0, bottom], two_b.at[k, 0, 1], near(axis, 1), marks[2])
        copies.wait(marks[0], two_a.at[k, 0])
        grad[k, 1, 0, 0:128] = grad[k, 1, 0, 0:128] + two_a[k, 0]
        copies.send(grad.at[k, 1, 0, top], two_b.at[k, 0, 0], near(axis, 1), marks[2])

    def two_minus(k):
        axis, marks = axes[k][1], pending["two", k]
        copies.send(grad.at[k, 3, 0, top], two_b.at[k, 1, 0], near(axis, 3), marks[2])
        copies.wait(marks[1], two_a.at[k, 1])
        grad[k, 3, 0, 128:256] = grad[k, 3, 0, 128:256] + two_a[k, 1]
        copies.send(grad.at[k, 3, 0, bottom], two_b.at[k, 1, 1], near(axis, 3), marks[2])

    def two_finish(k):
        copies.wait(pending["two", k][2], two_b.at[k])
        top_sum = grad[k, 0, 0, 0:128] + (two_b[k, 0, 0] + two_b[k, 1, 0])
        bottom_sum = grad[k, 0, 0, 128:256] + (two_b[k, 0, 1] + two_b[k, 1, 1])
        return jnp.concatenate([top_sum, bottom_sum], axis=0)

    def low_rows(k, b, half=None):
        start = lax.rem(coord[axes[k][0]] + b, 4) * 64
        if half is None:
            return pl.ds(pl.multiple_of(start, 64), 64)
        return pl.ds(pl.multiple_of(start + 32 * half, 32), 32)

    def low_piece(k, a):
        first, second = axes[k]
        return pl.ds(pl.multiple_of(coord[first] * 64 + lax.rem(coord[second] + a, 4) * 16, 16), 16)

    def low_start(k):
        far, plus, minus = ([low_t.at[k, low_rows(k, b, half)] for half in range(2)] for b in (2, 1, 3))
        opening(("low", k), axes[k][0], far, minus, plus, low_a.at[k], low_b.at[k])

    def low_forward(k):
        axis, marks = axes[k][0], pending["low", k]
        copies.wait(marks[0], low_a.at[k, 0])
        rows = low_rows(k, 1, 0)
        low_t[k, rows] = low_t[k, rows] + low_a[k, 0]
        copies.send(low_t.at[k, rows], low_b.at[k, 0, 0], near(axis, 1), marks[2])
        copies.wait(marks[1], low_a.at[k, 1])
        rows = low_rows(k, 3, 1)
        low_t[k, rows] = low_t[k, rows] + low_a[k, 1]
        copies.send(low_t.at[k, rows], low_b.at[k, 1, 1], near(axis, 3), marks[2])

    def low_second(k):
        copies.wait(pending["low", k][2], low_b.at[k])
        for half in range(2):
            rows = low_rows(k, 0, half)
            low_t[k, rows] = low_t[k, rows] + (low_b[k, 0, half] + low_b[k, 1, half])
        mark = pending["low2", k] = copies.landing()
        for a in (2, 1, 3):
            copies.send(low_t.at[k, low_piece(k, a)], low_in.at[k, 3 - a], near(axes[k][1], a), mark)

    def low_third(k):
        copies.wait(pending["low2", k], low_in.at[k])
        rows = low_piece(k, 0)
        low_all[k, rows] = low_t[k, rows] + low_in[k, 0] + low_in[k, 1] + low_in[k, 2]
        mark = pending["low3", k] = copies.landing()
        for a in (2, 1, 3):
            copies.send(low_all.at[k, rows], low_all.at[k, rows], near(axes[k][1], a), mark)

    def low_fourth(k):
        copies.wait(pending["low3", k], low_all.at[k, pl.ds(0, 48)])
        axis, rows = axes[k][0], low_rows(k, 0)
        marks = pending["low4", k] = [copies.landing() for _ in range(3)]
        copies.send(low_all.at[k, rows], low_all.at[k, rows], near(axis, 1), marks[0])
        copies.send(low_all.at[k, rows], low_all.at[k, rows], near(axis, 3), marks[1])

    def low_fifth(k):
        axis, marks = axes[k][0], pending["low4", k]
        copies.wait(marks[0], low_all.at[k, pl.ds(0, 64)])
        rows = low_rows(k, 3, 0)
        copies.send(low_all.at[k, rows], low_all.at[k, rows], near(axis, 1), marks[2])
        copies.wait(marks[1], low_all.at[k, pl.ds(0, 64)])
        rows = low_rows(k, 1, 1)
        copies.send(low_all.at[k, rows], low_all.at[k, rows], near(axis, 3), marks[2])

    def gram(k):
        total = None
        for a in range(4):
            rows = fact[k, a]
            term = jnp.dot(rows.T, rows, preferred_element_type=F32)
            total = term if total is None else total + term
        for i, part in enumerate(halves(total, 2)):
            grams[k, i] = part

    def turn(k):
        mom1_t[k] = mom1[k].T
        mom2_t[k] = mom2[k].T

    def own_terms(k):
        rows = low_piece(k, 0)
        low = low_all[k, rows, :]
        first = 0.9 * mom1_t[k, rows, :] + 0.1 * low
        second = 0.95 * mom2_t[k, rows, :] + 0.05 * low * low
        normed = first / (jnp.sqrt(second) + 1e-06)
        stack = jnp.concatenate(halves(normed, 2) + halves(low, 2), axis=0)
        product = sum(jnp.dot(stack, grams[k, i], preferred_element_type=F32) for i in range(2))
        by_normed = product[0:16] + product[16:32]
        by_low = product[32:48] + product[48:64]
        pairs = ((normed, by_normed), (normed, low), (normed, by_low), (low, low), (low, by_low), (normed, normed))
        row = jnp.zeros((1, 128), F32)
        for i, (one, other) in enumerate(pairs):
            row = jnp.where(lane == 8 * k + i, jnp.sum(folded(one * other), keepdims=True), row)
        return row

    def moments(k):
        copies.wait(pending["low4", k][2], low_all.at[k, pl.ds(0, 64)])
        low = low_all[k].T
        first = 0.9 * mom1[k] + 0.1 * low
        second = 0.95 * mom2[k] + 0.05 * low * low
        out_1[k] = first
        out_2[k] = second
        normed = first / (jnp.sqrt(second) + 1e-06)
        mine = fact[k, 0, 0:128, :]
        own_p[k] = sum(jnp.dot(mine, part, preferred_element_type=F32) for part in halves(normed, 3))
        own_f[k] = own_g[k].T - sum(jnp.dot(mine, part, preferred_element_type=F32) for part in halves(low, 3))

    lane = lax.broadcasted_iota(jnp.int32, (1, 128), 1)
    both = range(2)
    c0, c1, c2, c3 = ORDER
    for k in both:
        transpose_right(k)
        local_grad(k, c0)
        if k == 0:
            pl.semaphore_wait(barrier, len(fs_peers) + len(tp_peers))
        one_start(k, c0)
    for k in both:
        local_grad(k, c1)
    for k in both:
        fact_in[k].wait()
        local_low(k, c0)
        one_forward(k, c0)
        one_start(k, c1)
    for k in both:
        local_low(k, c1)
    for k in both:
        local_grad(k, c2)
        local_low(k, c2)
        one_forward(k, c1)
    for k in both:
        local_grad(k, c3)
        local_low(k, c3)
        low_start(k)
        one_start(k, c2)
    for k in both:
        one_finish(k, c0)
        two_start(k)
    for k in both:
        gram(k)
    for k in both:
        low_forward(k)
        one_start(k, c3)
    for k in both:
        one_forward(k, c2)
    mom1_in.wait()
    mom2_in.wait()
    wts_in.wait()
    for k in both:
        turn(k)
    for k in both:
        low_second(k)
    for k in both:
        one_finish(k, c1)
        two_plus(k)
    for k in both:
        one_forward(k, c3)
    for k in both:
        low_third(k)
    for k in both:
        one_finish(k, c2)
        two_minus(k)
    row = own_terms(0) + own_terms(1)
    for k in both:
        one_finish(k, c3)
    for k in both:
        own = two_finish(k)
        own_g[k] = own
        row = jnp.where(lane == 8 * k + 6, jnp.sum(folded(own * own), keepdims=True), row)
    pair_own[0:1, :] = row
    pair_mark, tot_mark = copies.landing(), copies.landing()
    first_row = pl.ds(0, 1)
    copies.send(pair_own.at[first_row], pair_in.at[first_row], {C: lax.rem(c + 1, 2)}, pair_mark, SENDS - 1)
    copies.wait(pair_mark, pair_in.at[first_row])
    row = row + pair_in[0:1, :]
    tot_own[0:1, :] = row
    tot_in[63:64, :] = row
    for i, peer in enumerate(all_peers):
        copies.send(tot_own.at[first_row], tot_in.at[pl.ds(i, 1)], peer, tot_mark, SENDS - 1)
    for k in both:
        low_fourth(k)
    for k in both:
        low_fifth(k)
    for k in both:
        moments(k)
    copies.wait(tot_mark, tot_in.at[pl.ds(0, 63)])
    sums = folded(tot_in[...]).sum(axis=0, keepdims=True)
    total, ratios = None, []
    for k in both:
        part = [jnp.sum(jnp.where(lane == 8 * k + i, sums, 0.0), keepdims=True) for i in range(7)]
        ratio = jnp.sqrt(part[5]) / jnp.sqrt(part[3] + 1e-06)
        value = part[0] + 2.0 * ratio * (part[1] - part[2]) + ratio * ratio * (part[6] - 2.0 * part[3] + part[4])
        total = value if total is None else total + value
        ratios.append(ratio)
    scale = lax.rsqrt(jnp.maximum(total, 0.0) / (2.0 * 2048 * 2048) + 1e-06)

    for k in range(2):
        value = (own_p[k] + ratios[k] * own_f[k]) * scale
        out_u[k] = value
        value = wts[k] - 0.02 * value
        out_w[k] = value
        gathered[k, 0, 0] = value.astype(BF16)

    upper, lower = pl.ds(0, 64), pl.ds(64, 64)

    def spread(k, b):
        marks = pending["w", k, b] = [copies.landing() for _ in range(3)]
        copies.send(gathered.at[k, 0, b], gathered.at[k, 3, b], near(axes[k][1], 1), marks[0])
        copies.send(gathered.at[k, 0, b], gathered.at[k, 1, b], near(axes[k][1], 3), marks[1])

    def relay(k, b):
        marks = pending["w", k, b]
        copies.wait(marks[0], gathered.at[k, 3, b])
        copies.send(gathered.at[k, 3, b, upper], gathered.at[k, 2, b, upper], near(axes[k][1], 1), marks[2])
        copies.wait(marks[1], gathered.at[k, 1, b])
        copies.send(gathered.at[k, 1, b, lower], gathered.at[k, 2, b, lower], near(axes[k][1], 3), marks[2])

    def land(k, b):
        copies.wait(pending["w", k, b][2], gathered.at[k, 2, b])

    def v_start(k):
        marks = pending["v", k] = [copies.landing() for _ in range(3)]
        copies.send(gathered.at[k, 0, 0], gathered.at[k, 0, 3], near(axes[k][0], 1), marks[0])
        copies.send(gathered.at[k, 0, 0], gathered.at[k, 0, 1], near(axes[k][0], 3), marks[1])

    def v_forward(k):
        marks = pending["v", k]
        copies.wait(marks[0], gathered.at[k, 0, 3])
        copies.send(gathered.at[k, 0, 3, upper], gathered.at[k, 0, 2, upper], near(axes[k][0], 1), marks[2])
        copies.wait(marks[1], gathered.at[k, 0, 1])
        copies.send(gathered.at[k, 0, 1, lower], gathered.at[k, 0, 2, lower], near(axes[k][0], 3), marks[2])

    def v_finish(k):
        copies.wait(pending["v", k][2], gathered.at[k, 0, 2])

    for k in both:
        v_start(k)
    for k in both:
        spread(k, 0)
    for k in both:
        v_forward(k)
    for b in (3, 1):
        for k in both:
            spread(k, b)
    for k in both:
        relay(k, 0)
    for k in both:
        v_finish(k)
        spread(k, 2)
    for b in (3, 1, 2):
        for k in both:
            relay(k, b)
    for b in (0, 3, 1, 2):
        for k in both:
            land(k, b)
    copies.wait_sent()
    pltpu.make_async_copy(tot_in, tot_in, send_sems.at[SENDS - 1]).wait()


def write_out(
    out_w, out_u, out_1, out_2, gathered, new_weights, update, new_first, new_second, weight_copy, sems
):
    z, x = lax.axis_index(Z), lax.axis_index(X)
    pairs = []
    for a in range(4):
        for b in range(4):
            for k in range(2):
                dz, dx = (a, b) if k == 0 else (b, a)
                block = lax.rem(z + dz, 4) * 4 + lax.rem(x + dx, 4)
                rows = pl.ds(pl.multiple_of(block * 128, 128), 128)
                pairs.append((gathered.at[k, a, b], weight_copy.at[k, rows, :]))
    for src, dst in pairs:
        pltpu.make_async_copy(src, dst, sems.at[0]).start()
    pairs = ((out_1, new_first), (out_2, new_second), (out_w, new_weights), (out_u, update))
    copies = [pltpu.make_async_copy(*pair, sems.at[1 + i]) for i, pair in enumerate(pairs)]
    for copy in copies:
        copy.start()
    for copy in copies:
        copy.wait()
    pltpu.make_async_copy(gathered, gathered, sems.at[0]).wait()


def per_device(*args):
    any_space = pl.BlockSpec(memory_space=pl.ANY)
    vmem_space = pl.BlockSpec(memory_space=pltpu.VMEM)
    held = (
        ((2, 128, 256), F32),
        ((2, 128, 256), F32),
        ((2, 256, 256), F32),
        ((2, 256, 256), F32),
        ((2, 4, 4, 128, 256), BF16),
    )
    dma = pltpu.SemaphoreType.DMA
    results = pl.pallas_call(
        kernel,
        name="step",
        out_shape=[pltpu.VMEM(*shape) for shape in held],
        in_specs=[any_space] * 8,
        out_specs=[vmem_space] * 5,
        scratch_shapes=[
            pltpu.VMEM((2, 4, 2560, 512), BF16),
            pltpu.VMEM((2, 2560, 256), BF16),
            pltpu.VMEM((2, 256, 2560), BF16),
            pltpu.VMEM((2, 4, 512, 256), BF16),
            pltpu.VMEM((2, 4, 4, 256, 128), F32),
            pltpu.VMEM((2, 4, 2, 128, 128), F32),
            pltpu.VMEM((2, 4, 2, 2, 128, 128), F32),
            pltpu.VMEM((2, 2, 128, 128), F32),
            pltpu.VMEM((2, 2, 2, 128, 128), F32),
            pltpu.VMEM((2, 256, 256), F32),
            pltpu.VMEM((2, 2, 32, 256), F32),
            pltpu.VMEM((2, 2, 2, 32, 256), F32),
            pltpu.VMEM((2, 3, 16, 256), F32),
            pltpu.VMEM((2, 256, 256), F32),
            pltpu.VMEM((2, 128, 256), F32),
            pltpu.VMEM((2, 256, 256), F32),
            pltpu.VMEM((2, 256, 256), F32),
            pltpu.VMEM((2, 128, 256), F32),
            pltpu.VMEM((2, 128, 256), F32),
            pltpu.VMEM((2, 256, 128), F32),
            pltpu.VMEM((2, 2, 256, 256), BF16),
            pltpu.VMEM((2, 256, 256), F32),
            pltpu.VMEM((2, 256, 256), F32),
            pltpu.VMEM((8, 128), F32),
            pltpu.VMEM((8, 128), F32),
            pltpu.VMEM((8, 128), F32),
            pltpu.VMEM((64, 128), F32),
            dma((LOADS,)),
            dma((SENDS,)),
            dma((LANDINGS,)),
        ],
        compiler_params=pltpu.CompilerParams(
            collective_id=0, has_side_effects=True, vmem_limit_bytes=60 * 1024 * 1024
        ),
    )(*args)
    return pl.pallas_call(
        write_out,
        name="write_out",
        out_shape=[jax.ShapeDtypeStruct(shape, kind) for shape, kind in held[:4]]
        + [jax.ShapeDtypeStruct((2, 2048, 256), BF16)],
        in_specs=[vmem_space] * 5,
        out_specs=[any_space] * 5,
        scratch_shapes=[dma((5,))],
        compiler_params=pltpu.CompilerParams(vmem_limit_bytes=1024 * 1024),
    )(*results)


def solution(mesh):
    finer = Mesh(mesh.devices.reshape(4, 4, 4, 2), (Z, X, Y, C))
    in_specs = (
        P(FS, None),
        P(FS, None),
        P(FS, TP),
        P(FS, TP),
        P(None, FS, TP),
        P(),
        P(None, None, TP),
        P(None, None, TP),
    )
    out_specs = (
        P(None, FS, TP),
        P(None, FS, TP),
        P(None, None, TP),
        P(None, None, TP),
        P(None, None, TP),
    )
    return jax.shard_map(per_device, mesh=finer, in_specs=in_specs, out_specs=out_specs, check_vma=False)
```

```python
import math

import jax
import jax.numpy as jnp
from jax import lax
from jax.experimental import pallas as pl
from jax.experimental.pallas import tpu as pltpu
from jax.sharding import Mesh
from jax.sharding import PartitionSpec as P

Z, X, Y, C = "fs_0", "fs_1", "tp_0", "tp_1"
FS, TP = (Z, X), (Y, C)
MESH = pl.DeviceIdType.MESH
F32, BF16 = jnp.float32, jnp.bfloat16
ORDER = (2, 1, 3, 0)


class Copies:
    def __init__(self, send_sems, recv_sems, spare):
        self.send_sems, self.recv_sems, self.spare = send_sems, recv_sems, spare
        self.landings, self.sent = 0, [0]

    def landing(self):
        self.landings += 1
        return self.landings - 1

    def send(self, src, dst, device, landing, own=None):
        size = math.prod(src.shape) * src.dtype.itemsize // 1024
        if own is None:
            if self.sent[-1] + size > self.spare.shape[0]:
                self.sent.append(0)
            self.sent[-1] += size
        pltpu.make_async_remote_copy(
            src_ref=src,
            dst_ref=dst,
            send_sem=self.send_sems.at[len(self.sent) - 1 if own is None else own],
            recv_sem=self.recv_sems.at[landing],
            device_id=device,
            device_id_type=MESH,
        ).start()

    def wait(self, landing, place):
        pltpu.make_async_copy(place, place, self.recv_sems.at[landing]).wait()

    def wait_sent(self):
        for index, size in enumerate(self.sent):
            rows = self.spare.at[pl.ds(0, size)]
            pltpu.make_async_copy(rows, rows, self.send_sems.at[index]).wait()


SENDS, LANDINGS, LOADS = 4, 84, 15


def halves(value, terms):
    out = []
    for _ in range(terms - 1):
        part = value.astype(BF16)
        out.append(part)
        value = value - part.astype(F32)
    out.append(value.astype(BF16))
    return out


def folded(value):
    rows, cols = value.shape
    total = value[:, 0:128]
    for start in range(128, cols, 128):
        total = total + value[:, start : start + 128]
    return total.reshape(rows // 8, 8, 128).sum(axis=0)


def kernel(
    layer_inputs, output_cot, query_cot, head_outputs, weights, factors, first_moment, second_moment,
    out_w, out_u, out_1, out_2, gathered,
    left, right, right_t, fact, grad, one_a, one_b, two_a, two_b,
    low_t, low_a, low_b, low_in, low_all, wts, mom1, mom2,
    own_p, own_f, own_g, grams, mom1_t, mom2_t, pair_own, pair_in, tot_own, tot_in,
    load_sems, send_sems, recv_sems,
):
    z, x, y, c = (lax.axis_index(name) for name in (Z, X, Y, C))
    lefts, rights = (layer_inputs, output_cot), (query_cot, head_outputs)
    coord = {Z: z, X: x, Y: y, C: c}
    axes = ((X, Z), (Z, X))

    def near(axis, delta):
        return {axis: lax.rem(coord[axis] + delta, 4)}

    def place(k, a, b):
        first, second = axes[k]
        at = {first: lax.rem(coord[first] + b, 4), second: lax.rem(coord[second] + a, 4)}
        return at[Z] * 4 + at[X]

    loads = []

    def load(pairs, whole):
        sem = load_sems.at[len(loads)]
        for src, dst in pairs:
            pltpu.make_async_copy(src, dst, sem).start()
        loads.append(pltpu.make_async_copy(whole, whole, sem))
        return loads[-1]

    def load_left(k, a):
        pairs = []
        for b in range(4):
            cols = pl.ds(pl.multiple_of(place(k, a, b) * 128, 128), 128)
            pairs.append((lefts[k].at[:, cols], left.at[k, a, :, pl.ds(128 * b, 128)]))
        return load(pairs, left.at[k, a])

    def load_factors(k):
        pairs = []
        for a in range(4):
            for b in range(4):
                rows = pl.ds(pl.multiple_of(place(k, a, b) * 128, 128), 128)
                pairs.append((factors.at[k, rows, :], fact.at[k, a, pl.ds(128 * b, 128), :]))
        return load(pairs, fact.at[k])

    right_in, left_in, fact_in = [None] * 2, {}, [None] * 2
    for k in range(2):
        right_in[k] = load([(rights[k], right.at[k])], right.at[k])
        left_in[k, ORDER[0]] = load_left(k, ORDER[0])
    for k in range(2):
        left_in[k, ORDER[1]] = load_left(k, ORDER[1])
    for k in range(2):
        fact_in[k] = load_factors(k)
    for a in ORDER[2:]:
        for k in range(2):
            left_in[k, a] = load_left(k, a)
    mom1_in = load([(first_moment, mom1)], mom1)
    mom2_in = load([(second_moment, mom2)], mom2)
    wts_in = load([(weights, wts)], wts)

    barrier = pltpu.get_barrier_semaphore()
    fs_peers = [
        {Z: lax.rem(z + dz, 4), X: lax.rem(x + dx, 4)} for dz in range(4) for dx in range(4) if dz or dx
    ]
    tp_peers = [
        {Y: lax.rem(y + dy, 4), C: lax.rem(c + dc, 2)} for dy in range(4) for dc in range(2) if dy or dc
    ]
    all_peers = [
        {Z: lax.rem(z + dz, 4), X: lax.rem(x + dx, 4), Y: lax.rem(y + dy, 4)}
        for dz in ORDER
        for dx in ORDER
        for dy in ORDER
        if dz or dx or dy
    ]
    for peer in fs_peers + tp_peers:
        pl.semaphore_signal(barrier, inc=1, device_id=peer, device_id_type=MESH)

    copies = Copies(send_sems, recv_sems, left.at[0, 0])
    top, bottom = pl.ds(0, 128), pl.ds(128, 128)

    def transpose_right(k):
        right_in[k].wait()
        for start in range(0, 2560, 256):
            right_t[k, :, start : start + 256] = right[k, start : start + 256, :].T

    def local_grad(k, a):
        left_in[k, a].wait()
        value = jnp.dot(right_t[k], left[k, a], preferred_element_type=F32)
        for b in range(4):
            grad[k, a, b] = value[:, 128 * b : 128 * b + 128]

    def local_low(k, a):
        total = None
        value = jnp.concatenate([grad[k, a, b] for b in range(4)], axis=1)
        for part in halves(value, 2):
            term = jnp.dot(part, fact[k, a], preferred_element_type=F32)
            total = term if total is None else total + term
        if a == ORDER[0]:
            low_t[k] = total
        else:
            low_t[k] = low_t[k] + total

    pending = {}

    def opening(key, axis, far, minus, plus, into_a, into_b):
        marks = pending[key] = [copies.landing() for _ in range(3)]
        copies.send(far[0], into_a.at[0], near(axis, 1), marks[0])
        copies.send(far[1], into_a.at[1], near(axis, 3), marks[1])
        copies.send(plus[1], into_b.at[0, 1], near(axis, 1), marks[2])
        copies.send(minus[0], into_b.at[1, 0], near(axis, 3), marks[2])

    def one_start(k, a):
        far, plus, minus = ((grad.at[k, a, b, top], grad.at[k, a, b, bottom]) for b in (2, 1, 3))
        opening(("one", k, a), axes[k][0], far, minus, plus, one_a.at[k, a], one_b.at[k, a])

    def one_forward(k, a):
        axis, marks = axes[k][0], pending["one", k, a]
        copies.wait(marks[0], one_a.at[k, a, 0])
        grad[k, a, 1, 0:128] = grad[k, a, 1, 0:128] + one_a[k, a, 0]
        copies.send(grad.at[k, a, 1, top], one_b.at[k, a, 0, 0], near(axis, 1), marks[2])
        copies.wait(marks[1], one_a.at[k, a, 1])
        grad[k, a, 3, 128:256] = grad[k, a, 3, 128:256] + one_a[k, a, 1]
        copies.send(grad.at[k, a, 3, bottom], one_b.at[k, a, 1, 1], near(axis, 3), marks[2])

    def one_finish(k, a):
        copies.wait(pending["one", k, a][2], one_b.at[k, a])
        grad[k, a, 0, 0:128] = grad[k, a, 0, 0:128] + (one_b[k, a, 0, 0] + one_b[k, a, 1, 0])
        grad[k, a, 0, 128:256] = grad[k, a, 0, 128:256] + (one_b[k, a, 0, 1] + one_b[k, a, 1, 1])

    def two_start(k):
        axis = axes[k][1]
        marks = pending["two", k] = [copies.landing() for _ in range(3)]
        copies.send(grad.at[k, 2, 0, top], two_a.at[k, 0], near(axis, 1), marks[0])
        copies.send(grad.at[k, 2, 0, bottom], two_a.at[k, 1], near(axis, 3), marks[1])

    def two_plus(k):
        axis, marks = axes[k][1], pending["two", k]
        copies.send(grad.at[k, 1, 0, bottom], two_b.at[k, 0, 1], near(axis, 1), marks[2])
        copies.wait(marks[0], two_a.at[k, 0])
        grad[k, 1, 0, 0:128] = grad[k, 1, 0, 0:128] + two_a[k, 0]
        copies.send(grad.at[k, 1, 0, top], two_b.at[k, 0, 0], near(axis, 1), marks[2])

    def two_minus(k):
        axis, marks = axes[k][1], pending["two", k]
        copies.send(grad.at[k, 3, 0, top], two_b.at[k, 1, 0], near(axis, 3), marks[2])
        copies.wait(marks[1], two_a.at[k, 1])
        grad[k, 3, 0, 128:256] = grad[k, 3, 0, 128:256] + two_a[k, 1]
        copies.send(grad.at[k, 3, 0, bottom], two_b.at[k, 1, 1], near(axis, 3), marks[2])

    def two_finish(k):
        copies.wait(pending["two", k][2], two_b.at[k])
        top_sum = grad[k, 0, 0, 0:128] + (two_b[k, 0, 0] + two_b[k, 1, 0])
        bottom_sum = grad[k, 0, 0, 128:256] + (two_b[k, 0, 1] + two_b[k, 1, 1])
        return jnp.concatenate([top_sum, bottom_sum], axis=0)

    def low_rows(k, b, half=None):
        start = lax.rem(coord[axes[k][0]] + b, 4) * 64
        if half is None:
            return pl.ds(pl.multiple_of(start, 64), 64)
        return pl.ds(pl.multiple_of(start + 32 * half, 32), 32)

    def low_piece(k, a):
        first, second = axes[k]
        return pl.ds(pl.multiple_of(coord[first] * 64 + lax.rem(coord[second] + a, 4) * 16, 16), 16)

    def low_start(k):
        far, plus, minus = ([low_t.at[k, low_rows(k, b, half)] for half in range(2)] for b in (2, 1, 3))
        opening(("low", k), axes[k][0], far, minus, plus, low_a.at[k], low_b.at[k])

    def low_forward(k):
        axis, marks = axes[k][0], pending["low", k]
        copies.wait(marks[0], low_a.at[k, 0])
        rows = low_rows(k, 1, 0)
        low_t[k, rows] = low_t[k, rows] + low_a[k, 0]
        copies.send(low_t.at[k, rows], low_b.at[k, 0, 0], near(axis, 1), marks[2])
        copies.wait(marks[1], low_a.at[k, 1])
        rows = low_rows(k, 3, 1)
        low_t[k, rows] = low_t[k, rows] + low_a[k, 1]
        copies.send(low_t.at[k, rows], low_b.at[k, 1, 1], near(axis, 3), marks[2])

    def low_second(k):
        copies.wait(pending["low", k][2], low_b.at[k])
        for half in range(2):
            rows = low_rows(k, 0, half)
            low_t[k, rows] = low_t[k, rows] + (low_b[k, 0, half] + low_b[k, 1, half])
        rows, slot = low_rows(k, 0), coord[axes[k][1]]
        low_in[k, slot] = low_t[k, rows]
        mark = pending["low2", k] = copies.landing()
        for a in (2, 1, 3):
            copies.send(low_t.at[k, rows], low_in.at[k, slot], near(axes[k][1], a), mark)

    def low_third(k):
        copies.wait(pending["low2", k], low_in.at[k, pl.ds(0, 3)])
        low_all[k, low_rows(k, 0)] = ((low_in[k, 0] + low_in[k, 1]) + low_in[k, 2]) + low_in[k, 3]

    def low_fourth(k):
        axis, rows = axes[k][0], low_rows(k, 0)
        marks = pending["low4", k] = [copies.landing() for _ in range(3)]
        copies.send(low_all.at[k, rows], low_all.at[k, rows], near(axis, 1), marks[0])
        copies.send(low_all.at[k, rows], low_all.at[k, rows], near(axis, 3), marks[1])

    def low_fifth(k):
        axis, marks = axes[k][0], pending["low4", k]
        copies.wait(marks[0], low_all.at[k, pl.ds(0, 64)])
        rows = low_rows(k, 3, 0)
        copies.send(low_all.at[k, rows], low_all.at[k, rows], near(axis, 1), marks[2])
        copies.wait(marks[1], low_all.at[k, pl.ds(0, 64)])
        rows = low_rows(k, 1, 1)
        copies.send(low_all.at[k, rows], low_all.at[k, rows], near(axis, 3), marks[2])

    def gram(k):
        total = None
        for a in range(4):
            rows = fact[k, a]
            term = jnp.dot(rows.T, rows, preferred_element_type=F32)
            total = term if total is None else total + term
        for i, part in enumerate(halves(total, 2)):
            grams[k, i] = part

    def turn(k):
        mom1_t[k] = mom1[k].T
        mom2_t[k] = mom2[k].T

    def own_terms(k):
        rows = low_piece(k, 0)
        low = low_all[k, rows, :]
        first = 0.9 * mom1_t[k, rows, :] + 0.1 * low
        second = 0.95 * mom2_t[k, rows, :] + 0.05 * low * low
        normed = first / (jnp.sqrt(second) + 1e-06)
        stack = jnp.concatenate(halves(normed, 2) + halves(low, 2), axis=0)
        product = sum(jnp.dot(stack, grams[k, i], preferred_element_type=F32) for i in range(2))
        by_normed = product[0:16] + product[16:32]
        by_low = product[32:48] + product[48:64]
        pairs = ((normed, by_normed), (normed, low), (normed, by_low), (low, low), (low, by_low), (normed, normed))
        row = jnp.zeros((1, 128), F32)
        for i, (one, other) in enumerate(pairs):
            row = jnp.where(lane == 8 * k + i, jnp.sum(folded(one * other), keepdims=True), row)
        return row

    def moments(k):
        copies.wait(pending["low4", k][2], low_all.at[k, pl.ds(0, 64)])
        low = low_all[k].T
        first = 0.9 * mom1[k] + 0.1 * low
        second = 0.95 * mom2[k] + 0.05 * low * low
        out_1[k] = first
        out_2[k] = second
        normed = first / (jnp.sqrt(second) + 1e-06)
        mine = fact[k, 0, 0:128, :]
        own_p[k] = sum(jnp.dot(mine, part, preferred_element_type=F32) for part in halves(normed, 3))
        own_f[k] = own_g[k].T - sum(jnp.dot(mine, part, preferred_element_type=F32) for part in halves(low, 3))

    lane = lax.broadcasted_iota(jnp.int32, (1, 128), 1)
    both = range(2)
    c0, c1, c2, c3 = ORDER
    for k in both:
        transpose_right(k)
        local_grad(k, c0)
        if k == 0:
            pl.semaphore_wait(barrier, len(fs_peers) + len(tp_peers))
        one_start(k, c0)
    for k in both:
        local_grad(k, c1)
    for k in both:
        fact_in[k].wait()
        local_low(k, c0)
        one_forward(k, c0)
        one_start(k, c1)
    for k in both:
        local_low(k, c1)
    for k in both:
        local_grad(k, c2)
        local_low(k, c2)
        one_forward(k, c1)
    for k in both:
        local_grad(k, c3)
        local_low(k, c3)
        low_start(k)
        one_start(k, c2)
    for k in both:
        one_finish(k, c0)
        two_start(k)
    for k in both:
        gram(k)
    for k in both:
        low_forward(k)
        one_start(k, c3)
    for k in both:
        one_forward(k, c2)
    mom1_in.wait()
    mom2_in.wait()
    wts_in.wait()
    for k in both:
        turn(k)
    for k in both:
        low_second(k)
    for k in both:
        one_finish(k, c1)
        two_plus(k)
    for k in both:
        one_forward(k, c3)
    for k in both:
        one_finish(k, c2)
        two_minus(k)
    for k in both:
        low_third(k)
        low_fourth(k)
    row = own_terms(0) + own_terms(1)
    for k in both:
        one_finish(k, c3)
    for k in both:
        own = two_finish(k)
        own_g[k] = own
        row = jnp.where(lane == 8 * k + 6, jnp.sum(folded(own * own), keepdims=True), row)
    pair_own[0:1, :] = row
    pair_mark, tot_mark = copies.landing(), copies.landing()
    first_row = pl.ds(0, 1)
    copies.send(pair_own.at[first_row], pair_in.at[first_row], {C: lax.rem(c + 1, 2)}, pair_mark, SENDS - 1)
    copies.wait(pair_mark, pair_in.at[first_row])
    row = row + pair_in[0:1, :]
    tot_own[0:1, :] = row
    tot_in[63:64, :] = row
    for i, peer in enumerate(all_peers):
        copies.send(tot_own.at[first_row], tot_in.at[pl.ds(i, 1)], peer, tot_mark, SENDS - 1)
    for k in both:
        low_fifth(k)
    for k in both:
        moments(k)
    copies.wait(tot_mark, tot_in.at[pl.ds(0, 63)])
    sums = folded(tot_in[...]).sum(axis=0, keepdims=True)
    total, ratios = None, []
    for k in both:
        part = [jnp.sum(jnp.where(lane == 8 * k + i, sums, 0.0), keepdims=True) for i in range(7)]
        ratio = jnp.sqrt(part[5]) / jnp.sqrt(part[3] + 1e-06)
        value = part[0] + 2.0 * ratio * (part[1] - part[2]) + ratio * ratio * (part[6] - 2.0 * part[3] + part[4])
        total = value if total is None else total + value
        ratios.append(ratio)
    scale = lax.rsqrt(jnp.maximum(total, 0.0) / (2.0 * 2048 * 2048) + 1e-06)

    for k in range(2):
        value = (own_p[k] + ratios[k] * own_f[k]) * scale
        out_u[k] = value
        value = wts[k] - 0.02 * value
        out_w[k] = value
        gathered[k, 0, 0] = value.astype(BF16)

    upper, lower = pl.ds(0, 64), pl.ds(64, 64)

    def by_halves(key, axis, block, plus, minus):
        marks = pending[key] = [copies.landing() for _ in range(5)]
        copies.send(block.at[upper], plus.at[upper], near(axis, 1), marks[0])
        copies.send(block.at[lower], minus.at[lower], near(axis, 3), marks[1])
        copies.send(block.at[lower], plus.at[lower], near(axis, 1), marks[3])
        copies.send(block.at[upper], minus.at[upper], near(axis, 3), marks[4])

    def pass_on(key, axis, plus, minus, far, whole):
        marks = pending[key]
        copies.wait(marks[0], plus if whole else plus.at[upper])
        copies.send(plus.at[upper], far.at[upper], near(axis, 1), marks[2])
        copies.wait(marks[1], minus if whole else minus.at[lower])
        copies.send(minus.at[lower], far.at[lower], near(axis, 3), marks[2])

    def spread(k, b):
        block, plus, minus, axis = gathered.at[k, 0, b], gathered.at[k, 3, b], gathered.at[k, 1, b], axes[k][1]
        if b == 2:
            by_halves(("w", k, b), axis, block, plus, minus)
        else:
            marks = pending["w", k, b] = [copies.landing() for _ in range(3)]
            copies.send(block, plus, near(axis, 1), marks[0])
            copies.send(block, minus, near(axis, 3), marks[1])

    def relay(k, b):
        plus, minus, far = gathered.at[k, 3, b], gathered.at[k, 1, b], gathered.at[k, 2, b]
        pass_on(("w", k, b), axes[k][1], plus, minus, far, b != 2)

    def land(k, b):
        marks = pending["w", k, b]
        if b == 2:
            copies.wait(marks[3], gathered.at[k, 3, b, lower])
            copies.wait(marks[4], gathered.at[k, 1, b, upper])
        copies.wait(marks[2], gathered.at[k, 2, b])

    def v_start(k):
        by_halves(("v", k), axes[k][0], gathered.at[k, 0, 0], gathered.at[k, 0, 3], gathered.at[k, 0, 1])

    def v_forward(k):
        pass_on(("v", k), axes[k][0], gathered.at[k, 0, 3], gathered.at[k, 0, 1], gathered.at[k, 0, 2], False)

    def v_rest(k):
        copies.wait(pending["v", k][3], gathered.at[k, 0, 3, lower])
        copies.wait(pending["v", k][4], gathered.at[k, 0, 1, upper])

    def v_finish(k):
        copies.wait(pending["v", k][2], gathered.at[k, 0, 2])

    for k in both:
        v_start(k)
    for k in both:
        spread(k, 0)
    for k in both:
        v_forward(k)
    for k in both:
        v_rest(k)
    for b in (3, 1):
        for k in both:
            spread(k, b)
    for k in both:
        relay(k, 0)
    for k in both:
        v_finish(k)
        spread(k, 2)
    for b in (3, 1, 2):
        for k in both:
            relay(k, b)
    for b in (0, 3, 1, 2):
        for k in both:
            land(k, b)
    copies.wait_sent()
    pltpu.make_async_copy(tot_in, tot_in, send_sems.at[SENDS - 1]).wait()


def write_out(
    out_w, out_u, out_1, out_2, gathered, new_weights, update, new_first, new_second, weight_copy, sems
):
    z, x = lax.axis_index(Z), lax.axis_index(X)
    pairs = []
    for a in range(4):
        for b in range(4):
            for k in range(2):
                dz, dx = (a, b) if k == 0 else (b, a)
                block = lax.rem(z + dz, 4) * 4 + lax.rem(x + dx, 4)
                rows = pl.ds(pl.multiple_of(block * 128, 128), 128)
                pairs.append((gathered.at[k, a, b], weight_copy.at[k, rows, :]))
    for src, dst in pairs:
        pltpu.make_async_copy(src, dst, sems.at[0]).start()
    pairs = ((out_1, new_first), (out_2, new_second), (out_w, new_weights), (out_u, update))
    copies = [pltpu.make_async_copy(*pair, sems.at[1 + i]) for i, pair in enumerate(pairs)]
    for copy in copies:
        copy.start()
    for copy in copies:
        copy.wait()
    pltpu.make_async_copy(gathered, gathered, sems.at[0]).wait()


def per_device(*args):
    any_space = pl.BlockSpec(memory_space=pl.ANY)
    vmem_space = pl.BlockSpec(memory_space=pltpu.VMEM)
    held = (
        ((2, 128, 256), F32),
        ((2, 128, 256), F32),
        ((2, 256, 256), F32),
        ((2, 256, 256), F32),
        ((2, 4, 4, 128, 256), BF16),
    )
    dma = pltpu.SemaphoreType.DMA
    results = pl.pallas_call(
        kernel,
        name="step",
        out_shape=[pltpu.VMEM(*shape) for shape in held],
        in_specs=[any_space] * 8,
        out_specs=[vmem_space] * 5,
        scratch_shapes=[
            pltpu.VMEM((2, 4, 2560, 512), BF16),
            pltpu.VMEM((2, 2560, 256), BF16),
            pltpu.VMEM((2, 256, 2560), BF16),
            pltpu.VMEM((2, 4, 512, 256), BF16),
            pltpu.VMEM((2, 4, 4, 256, 128), F32),
            pltpu.VMEM((2, 4, 2, 128, 128), F32),
            pltpu.VMEM((2, 4, 2, 2, 128, 128), F32),
            pltpu.VMEM((2, 2, 128, 128), F32),
            pltpu.VMEM((2, 2, 2, 128, 128), F32),
            pltpu.VMEM((2, 256, 256), F32),
            pltpu.VMEM((2, 2, 32, 256), F32),
            pltpu.VMEM((2, 2, 2, 32, 256), F32),
            pltpu.VMEM((2, 4, 64, 256), F32),
            pltpu.VMEM((2, 256, 256), F32),
            pltpu.VMEM((2, 128, 256), F32),
            pltpu.VMEM((2, 256, 256), F32),
            pltpu.VMEM((2, 256, 256), F32),
            pltpu.VMEM((2, 128, 256), F32),
            pltpu.VMEM((2, 128, 256), F32),
            pltpu.VMEM((2, 256, 128), F32),
            pltpu.VMEM((2, 2, 256, 256), BF16),
            pltpu.VMEM((2, 256, 256), F32),
            pltpu.VMEM((2, 256, 256), F32),
            pltpu.VMEM((8, 128), F32),
            pltpu.VMEM((8, 128), F32),
            pltpu.VMEM((8, 128), F32),
            pltpu.VMEM((64, 128), F32),
            dma((LOADS,)),
            dma((SENDS,)),
            dma((LANDINGS,)),
        ],
        compiler_params=pltpu.CompilerParams(
            collective_id=0, has_side_effects=True, vmem_limit_bytes=60 * 1024 * 1024
        ),
    )(*args)
    return pl.pallas_call(
        write_out,
        name="write_out",
        out_shape=[jax.ShapeDtypeStruct(shape, kind) for shape, kind in held[:4]]
        + [jax.ShapeDtypeStruct((2, 2048, 256), BF16)],
        in_specs=[vmem_space] * 5,
        out_specs=[any_space] * 5,
        scratch_shapes=[dma((5,))],
        compiler_params=pltpu.CompilerParams(vmem_limit_bytes=1024 * 1024),
    )(*results)


def solution(mesh):
    finer = Mesh(mesh.devices.reshape(4, 4, 4, 2), (Z, X, Y, C))
    in_specs = (
        P(FS, None),
        P(FS, None),
        P(FS, TP),
        P(FS, TP),
        P(None, FS, TP),
        P(),
        P(None, None, TP),
        P(None, None, TP),
    )
    out_specs = (
        P(None, FS, TP),
        P(None, FS, TP),
        P(None, None, TP),
        P(None, None, TP),
        P(None, None, TP),
    )
    return jax.shard_map(per_device, mesh=finer, in_specs=in_specs, out_specs=out_specs, check_vma=False)
```

```python
import math

import jax
import jax.numpy as jnp
from jax import lax
from jax.experimental import pallas as pl
from jax.experimental.pallas import tpu as pltpu
from jax.sharding import Mesh
from jax.sharding import PartitionSpec as P

Z, X, Y, C = "fs_0", "fs_1", "tp_0", "tp_1"
FS, TP = (Z, X), (Y, C)
MESH = pl.DeviceIdType.MESH
F32, BF16 = jnp.float32, jnp.bfloat16
ORDER = (2, 1, 3, 0)


class Copies:
    def __init__(self, send_sems, recv_sems, spare):
        self.send_sems, self.recv_sems, self.spare = send_sems, recv_sems, spare
        self.landings, self.sent = 0, [0]

    def landing(self):
        self.landings += 1
        return self.landings - 1

    def send(self, src, dst, device, landing, own=None):
        size = math.prod(src.shape) * src.dtype.itemsize // 1024
        if own is None:
            if self.sent[-1] + size > self.spare.shape[0]:
                self.sent.append(0)
            self.sent[-1] += size
        pltpu.make_async_remote_copy(
            src_ref=src,
            dst_ref=dst,
            send_sem=self.send_sems.at[len(self.sent) - 1 if own is None else own],
            recv_sem=self.recv_sems.at[landing],
            device_id=device,
            device_id_type=MESH,
        ).start()

    def wait(self, landing, place):
        pltpu.make_async_copy(place, place, self.recv_sems.at[landing]).wait()

    def wait_sent(self):
        for index, size in enumerate(self.sent):
            rows = self.spare.at[pl.ds(0, size)]
            pltpu.make_async_copy(rows, rows, self.send_sems.at[index]).wait()


SENDS, LANDINGS, LOADS = 4, 46, 15


def halves(value, terms):
    out = []
    for _ in range(terms - 1):
        part = value.astype(BF16)
        out.append(part)
        value = value - part.astype(F32)
    out.append(value.astype(BF16))
    return out


def folded(value):
    rows, cols = value.shape
    total = value[:, 0:128]
    for start in range(128, cols, 128):
        total = total + value[:, start : start + 128]
    return total.reshape(rows // 8, 8, 128).sum(axis=0)


def kernel(
    layer_inputs, output_cot, query_cot, head_outputs, weights, factors, first_moment, second_moment,
    out_w, out_u, out_1, out_2, gathered,
    left, right, right_t, fact, grad, one_a, one_b, two_a, two_b,
    low_t, low_a, low_b, low_in, low_all, wts, mom1, mom2,
    own_p, own_f, own_g, grams, mom1_t, mom2_t, pair_own, pair_in, tot_own, tot_in,
    load_sems, send_sems, recv_sems,
):
    z, x, y, c = (lax.axis_index(name) for name in (Z, X, Y, C))
    lefts, rights = (layer_inputs, output_cot), (query_cot, head_outputs)
    coord = {Z: z, X: x, Y: y, C: c}
    axes = ((X, Z), (Z, X))

    def near(axis, delta):
        return {axis: lax.rem(coord[axis] + delta, 4)}

    def place(k, a, b):
        first, second = axes[k]
        at = {first: lax.rem(coord[first] + b, 4), second: lax.rem(coord[second] + a, 4)}
        return at[Z] * 4 + at[X]

    loads = []

    def load(pairs, whole):
        sem = load_sems.at[len(loads)]
        for src, dst in pairs:
            pltpu.make_async_copy(src, dst, sem).start()
        loads.append(pltpu.make_async_copy(whole, whole, sem))
        return loads[-1]

    def load_left(k, a):
        pairs = []
        for b in range(4):
            cols = pl.ds(pl.multiple_of(place(k, a, b) * 128, 128), 128)
            pairs.append((lefts[k].at[:, cols], left.at[k, a, :, pl.ds(128 * b, 128)]))
        return load(pairs, left.at[k, a])

    def load_factors(k):
        pairs = []
        for a in range(4):
            for b in range(4):
                rows = pl.ds(pl.multiple_of(place(k, a, b) * 128, 128), 128)
                pairs.append((factors.at[k, rows, :], fact.at[k, a, pl.ds(128 * b, 128), :]))
        return load(pairs, fact.at[k])

    right_in, left_in, fact_in = [None] * 2, {}, [None] * 2
    for k in range(2):
        right_in[k] = load([(rights[k], right.at[k])], right.at[k])
        left_in[k, ORDER[0]] = load_left(k, ORDER[0])
    for k in range(2):
        left_in[k, ORDER[1]] = load_left(k, ORDER[1])
    for k in range(2):
        fact_in[k] = load_factors(k)
    for a in ORDER[2:]:
        for k in range(2):
            left_in[k, a] = load_left(k, a)
    mom1_in = load([(first_moment, mom1)], mom1)
    mom2_in = load([(second_moment, mom2)], mom2)
    wts_in = load([(weights, wts)], wts)

    barrier = pltpu.get_barrier_semaphore()
    fs_peers = [
        {Z: lax.rem(z + dz, 4), X: lax.rem(x + dx, 4)} for dz in range(4) for dx in range(4) if dz or dx
    ]
    tp_peers = [
        {Y: lax.rem(y + dy, 4), C: lax.rem(c + dc, 2)} for dy in range(4) for dc in range(2) if dy or dc
    ]
    all_peers = [
        {Z: lax.rem(z + dz, 4), X: lax.rem(x + dx, 4), Y: lax.rem(y + dy, 4)}
        for dz in ORDER
        for dx in ORDER
        for dy in ORDER
        if dz or dx or dy
    ]
    for peer in fs_peers + tp_peers:
        pl.semaphore_signal(barrier, inc=1, device_id=peer, device_id_type=MESH)

    copies = Copies(send_sems, recv_sems, left.at[0, 0])
    top, bottom = pl.ds(0, 128), pl.ds(128, 128)

    def transpose_right(k):
        right_in[k].wait()
        for start in range(0, 2560, 256):
            right_t[k, :, start : start + 256] = right[k, start : start + 256, :].T

    def local_grad(k, a):
        left_in[k, a].wait()
        value = jnp.dot(right_t[k], left[k, a], preferred_element_type=F32)
        for b in range(4):
            grad[k, a, b] = value[:, 128 * b : 128 * b + 128]

    def local_low(k, a):
        total = None
        value = jnp.concatenate([grad[k, a, b] for b in range(4)], axis=1)
        for part in halves(value, 2):
            term = jnp.dot(part, fact[k, a], preferred_element_type=F32)
            total = term if total is None else total + term
        if a == ORDER[0]:
            low_t[k] = total
        else:
            low_t[k] = low_t[k] + total

    pending = {}

    def opening(key, axis, far, minus, plus, into_a, into_b):
        marks = pending[key] = [copies.landing() for _ in range(3)]
        copies.send(far[0], into_a.at[0], near(axis, 1), marks[0])
        copies.send(far[1], into_a.at[1], near(axis, 3), marks[1])
        copies.send(plus[1], into_b.at[0, 1], near(axis, 1), marks[2])
        copies.send(minus[0], into_b.at[1, 0], near(axis, 3), marks[2])

    def one_start(k, a):
        far, plus, minus = ((grad.at[k, a, b, top], grad.at[k, a, b, bottom]) for b in (2, 1, 3))
        opening(("one", k, a), axes[k][0], far, minus, plus, one_a.at[k, a], one_b.at[k, a])

    def one_forward(k, a):
        axis, marks = axes[k][0], pending["one", k, a]
        copies.wait(marks[0], one_a.at[k, a, 0])
        grad[k, a, 1, 0:128] = grad[k, a, 1, 0:128] + one_a[k, a, 0]
        copies.send(grad.at[k, a, 1, top], one_b.at[k, a, 0, 0], near(axis, 1), marks[2])
        copies.wait(marks[1], one_a.at[k, a, 1])
        grad[k, a, 3, 128:256] = grad[k, a, 3, 128:256] + one_a[k, a, 1]
        copies.send(grad.at[k, a, 3, bottom], one_b.at[k, a, 1, 1], near(axis, 3), marks[2])

    def one_finish(k, a):
        copies.wait(pending["one", k, a][2], one_b.at[k, a])
        grad[k, a, 0, 0:128] = grad[k, a, 0, 0:128] + (one_b[k, a, 0, 0] + one_b[k, a, 1, 0])
        grad[k, a, 0, 128:256] = grad[k, a, 0, 128:256] + (one_b[k, a, 0, 1] + one_b[k, a, 1, 1])

    def two_start(k):
        axis = axes[k][1]
        marks = pending["two", k] = [copies.landing() for _ in range(3)]
        copies.send(grad.at[k, 2, 0, top], two_a.at[k, 0], near(axis, 1), marks[0])
        copies.send(grad.at[k, 2, 0, bottom], two_a.at[k, 1], near(axis, 3), marks[1])

    def two_plus(k):
        axis, marks = axes[k][1], pending["two", k]
        copies.send(grad.at[k, 1, 0, bottom], two_b.at[k, 0, 1], near(axis, 1), marks[2])
        copies.wait(marks[0], two_a.at[k, 0])
        grad[k, 1, 0, 0:128] = grad[k, 1, 0, 0:128] + two_a[k, 0]
        copies.send(grad.at[k, 1, 0, top], two_b.at[k, 0, 0], near(axis, 1), marks[2])

    def two_minus(k):
        axis, marks = axes[k][1], pending["two", k]
        copies.send(grad.at[k, 3, 0, top], two_b.at[k, 1, 0], near(axis, 3), marks[2])
        copies.wait(marks[1], two_a.at[k, 1])
        grad[k, 3, 0, 128:256] = grad[k, 3, 0, 128:256] + two_a[k, 1]
        copies.send(grad.at[k, 3, 0, bottom], two_b.at[k, 1, 1], near(axis, 3), marks[2])

    def two_finish(k):
        copies.wait(pending["two", k][2], two_b.at[k])
        top_sum = grad[k, 0, 0, 0:128] + (two_b[k, 0, 0] + two_b[k, 1, 0])
        bottom_sum = grad[k, 0, 0, 128:256] + (two_b[k, 0, 1] + two_b[k, 1, 1])
        return jnp.concatenate([top_sum, bottom_sum], axis=0)

    def low_rows(k, b, half=None):
        start = lax.rem(coord[axes[k][0]] + b, 4) * 64
        if half is None:
            return pl.ds(pl.multiple_of(start, 64), 64)
        return pl.ds(pl.multiple_of(start + 32 * half, 32), 32)

    def low_piece(k, a):
        first, second = axes[k]
        return pl.ds(pl.multiple_of(coord[first] * 64 + lax.rem(coord[second] + a, 4) * 16, 16), 16)

    def low_start(k):
        far, plus, minus = ([low_t.at[k, low_rows(k, b, half)] for half in range(2)] for b in (2, 1, 3))
        opening(("low", k), axes[k][0], far, minus, plus, low_a.at[k], low_b.at[k])

    def low_forward(k):
        axis, marks = axes[k][0], pending["low", k]
        copies.wait(marks[0], low_a.at[k, 0])
        rows = low_rows(k, 1, 0)
        low_t[k, rows] = low_t[k, rows] + low_a[k, 0]
        copies.send(low_t.at[k, rows], low_b.at[k, 0, 0], near(axis, 1), marks[2])
        copies.wait(marks[1], low_a.at[k, 1])
        rows = low_rows(k, 3, 1)
        low_t[k, rows] = low_t[k, rows] + low_a[k, 1]
        copies.send(low_t.at[k, rows], low_b.at[k, 1, 1], near(axis, 3), marks[2])

    def low_second(k):
        copies.wait(pending["low", k][2], low_b.at[k])
        for half in range(2):
            rows = low_rows(k, 0, half)
            low_t[k, rows] = low_t[k, rows] + (low_b[k, 0, half] + low_b[k, 1, half])
        rows, slot = low_rows(k, 0), coord[axes[k][1]]
        low_in[k, slot] = low_t[k, rows]
        mark = pending["low2", k] = copies.landing()
        for a in (2, 1, 3):
            copies.send(low_t.at[k, rows], low_in.at[k, slot], near(axes[k][1], a), mark)

    def low_third(k):
        copies.wait(pending["low2", k], low_in.at[k, pl.ds(0, 3)])
        low_all[k, low_rows(k, 0)] = ((low_in[k, 0] + low_in[k, 1]) + low_in[k, 2]) + low_in[k, 3]

    def low_fourth(k):
        axis, rows = axes[k][0], low_rows(k, 0)
        marks = pending["low4", k] = [copies.landing() for _ in range(3)]
        copies.send(low_all.at[k, rows], low_all.at[k, rows], near(axis, 1), marks[0])
        copies.send(low_all.at[k, rows], low_all.at[k, rows], near(axis, 3), marks[1])

    def low_fifth(k):
        axis, marks = axes[k][0], pending["low4", k]
        copies.wait(marks[0], low_all.at[k, pl.ds(0, 64)])
        rows = low_rows(k, 3, 0)
        copies.send(low_all.at[k, rows], low_all.at[k, rows], near(axis, 1), marks[2])
        copies.wait(marks[1], low_all.at[k, pl.ds(0, 64)])
        rows = low_rows(k, 1, 1)
        copies.send(low_all.at[k, rows], low_all.at[k, rows], near(axis, 3), marks[2])

    def gram(k):
        total = None
        for a in range(4):
            rows = fact[k, a]
            term = jnp.dot(rows.T, rows, preferred_element_type=F32)
            total = term if total is None else total + term
        for i, part in enumerate(halves(total, 2)):
            grams[k, i] = part

    def turn(k):
        mom1_t[k] = mom1[k].T
        mom2_t[k] = mom2[k].T

    def own_terms(k):
        rows = low_piece(k, 0)
        low = low_all[k, rows, :]
        first = 0.9 * mom1_t[k, rows, :] + 0.1 * low
        second = 0.95 * mom2_t[k, rows, :] + 0.05 * low * low
        normed = first / (jnp.sqrt(second) + 1e-06)
        stack = jnp.concatenate(halves(normed, 2) + halves(low, 2), axis=0)
        product = sum(jnp.dot(stack, grams[k, i], preferred_element_type=F32) for i in range(2))
        by_normed = product[0:16] + product[16:32]
        by_low = product[32:48] + product[48:64]
        pairs = ((normed, by_normed), (normed, low), (normed, by_low), (low, low), (low, by_low), (normed, normed))
        row = jnp.zeros((1, 128), F32)
        for i, (one, other) in enumerate(pairs):
            row = jnp.where(lane == 8 * k + i, jnp.sum(folded(one * other), keepdims=True), row)
        return row

    def moments(k):
        copies.wait(pending["low4", k][2], low_all.at[k, pl.ds(0, 64)])
        low = low_all[k].T
        first = 0.9 * mom1[k] + 0.1 * low
        second = 0.95 * mom2[k] + 0.05 * low * low
        out_1[k] = first
        out_2[k] = second
        normed = first / (jnp.sqrt(second) + 1e-06)
        mine = fact[k, 0, 0:128, :]
        own_p[k] = sum(jnp.dot(mine, part, preferred_element_type=F32) for part in halves(normed, 3))
        own_f[k] = own_g[k] - sum(jnp.dot(mine, part, preferred_element_type=F32) for part in halves(low, 3))

    lane = lax.broadcasted_iota(jnp.int32, (1, 128), 1)
    both = range(2)
    c0, c1, c2, c3 = ORDER
    for k in both:
        transpose_right(k)
        local_grad(k, c0)
        if k == 0:
            pl.semaphore_wait(barrier, len(fs_peers) + len(tp_peers))
        one_start(k, c0)
    for k in both:
        local_grad(k, c1)
    for k in both:
        fact_in[k].wait()
        local_low(k, c0)
        one_forward(k, c0)
        one_start(k, c1)
    for k in both:
        local_low(k, c1)
    for k in both:
        local_grad(k, c2)
        local_low(k, c2)
        one_forward(k, c1)
    for k in both:
        local_grad(k, c3)
        local_low(k, c3)
        low_start(k)
        one_start(k, c2)
    for k in both:
        one_finish(k, c0)
        two_start(k)
    for k in both:
        gram(k)
    for k in both:
        low_forward(k)
    for k in both:
        one_forward(k, c2)
        one_start(k, c3)
    mom1_in.wait()
    mom2_in.wait()
    wts_in.wait()
    for k in both:
        turn(k)
    for k in both:
        low_second(k)
    for k in both:
        one_finish(k, c1)
        two_plus(k)
    for k in both:
        one_forward(k, c3)
    for k in both:
        one_finish(k, c2)
        two_minus(k)
    for k in both:
        low_third(k)
        low_fourth(k)
    row = own_terms(0) + own_terms(1)
    for k in both:
        one_finish(k, c3)
    for k in both:
        own = two_finish(k)
        own_g[k] = own.T
        row = jnp.where(lane == 8 * k + 6, jnp.sum(folded(own * own), keepdims=True), row)
    pair_own[0:1, :] = row
    pair_mark, tot_mark = copies.landing(), copies.landing()
    first_row = pl.ds(0, 1)
    copies.send(pair_own.at[first_row], pair_in.at[first_row], {C: lax.rem(c + 1, 2)}, pair_mark, SENDS - 1)
    copies.wait(pair_mark, pair_in.at[first_row])
    row = row + pair_in[0:1, :]
    tot_own[0:1, :] = row
    tot_in[63:64, :] = row
    for i, peer in enumerate(all_peers):
        copies.send(tot_own.at[first_row], tot_in.at[pl.ds(i, 1)], peer, tot_mark, SENDS - 1)
    for k in both:
        low_fifth(k)
    for k in both:
        moments(k)
    copies.wait(tot_mark, tot_in.at[pl.ds(0, 63)])
    sums = folded(tot_in[...]).sum(axis=0, keepdims=True)
    total, ratios = None, []
    for k in both:
        part = [jnp.sum(jnp.where(lane == 8 * k + i, sums, 0.0), keepdims=True) for i in range(7)]
        ratio = jnp.sqrt(part[5]) / jnp.sqrt(part[3] + 1e-06)
        value = part[0] + 2.0 * ratio * (part[1] - part[2]) + ratio * ratio * (part[6] - 2.0 * part[3] + part[4])
        total = value if total is None else total + value
        ratios.append(ratio)
    scale = lax.rsqrt(jnp.maximum(total, 0.0) / (2.0 * 2048 * 2048) + 1e-06)

    for k in range(2):
        value = (own_p[k] + ratios[k] * own_f[k]) * scale
        out_u[k] = value
        value = wts[k] - 0.02 * value
        out_w[k] = value
        gathered[k, 0, 0] = value.astype(BF16)

    upper, lower = pl.ds(0, 64), pl.ds(64, 64)

    def by_halves(key, axis, block, plus, minus):
        marks = pending[key] = [copies.landing() for _ in range(5)]
        copies.send(block.at[upper], plus.at[upper], near(axis, 1), marks[0])
        copies.send(block.at[lower], minus.at[lower], near(axis, 3), marks[1])
        copies.send(block.at[lower], plus.at[lower], near(axis, 1), marks[3])
        copies.send(block.at[upper], minus.at[upper], near(axis, 3), marks[4])

    def pass_on(key, axis, plus, minus, far, whole):
        marks = pending[key]
        copies.wait(marks[0], plus if whole else plus.at[upper])
        copies.send(plus.at[upper], far.at[upper], near(axis, 1), marks[2])
        copies.wait(marks[1], minus if whole else minus.at[lower])
        copies.send(minus.at[lower], far.at[lower], near(axis, 3), marks[2])

    def spread(k, b):
        block, plus, minus, axis = gathered.at[k, 0, b], gathered.at[k, 3, b], gathered.at[k, 1, b], axes[k][1]
        if b == 2:
            by_halves(("w", k, b), axis, block, plus, minus)
        else:
            marks = pending["w", k, b] = [copies.landing() for _ in range(3)]
            copies.send(block, plus, near(axis, 1), marks[0])
            copies.send(block, minus, near(axis, 3), marks[1])

    def relay(k, b):
        plus, minus, far = gathered.at[k, 3, b], gathered.at[k, 1, b], gathered.at[k, 2, b]
        pass_on(("w", k, b), axes[k][1], plus, minus, far, b != 2)

    def land(k, b):
        marks = pending["w", k, b]
        if b == 2:
            copies.wait(marks[3], gathered.at[k, 3, b, lower])
            copies.wait(marks[4], gathered.at[k, 1, b, upper])
        copies.wait(marks[2], gathered.at[k, 2, b])

    def v_start(k):
        by_halves(("v", k), axes[k][0], gathered.at[k, 0, 0], gathered.at[k, 0, 3], gathered.at[k, 0, 1])

    def v_forward(k):
        pass_on(("v", k), axes[k][0], gathered.at[k, 0, 3], gathered.at[k, 0, 1], gathered.at[k, 0, 2], False)

    def v_rest(k):
        copies.wait(pending["v", k][3], gathered.at[k, 0, 3, lower])
        copies.wait(pending["v", k][4], gathered.at[k, 0, 1, upper])

    def v_finish(k):
        copies.wait(pending["v", k][2], gathered.at[k, 0, 2])

    copies.landings = 0
    for k in both:
        v_start(k)
    for k in both:
        spread(k, 0)
    for k in both:
        v_forward(k)
    for k in both:
        v_rest(k)
    for b in (3, 1):
        for k in both:
            spread(k, b)
    for k in both:
        relay(k, 0)
    for k in both:
        v_finish(k)
        spread(k, 2)
    for b in (3, 1, 2):
        for k in both:
            relay(k, b)
    for b in (0, 3, 1, 2):
        for k in both:
            land(k, b)
    copies.wait_sent()
    pltpu.make_async_copy(tot_in, tot_in, send_sems.at[SENDS - 1]).wait()


def write_out(
    out_w, out_u, out_1, out_2, gathered, new_weights, update, new_first, new_second, weight_copy, sems
):
    z, x = lax.axis_index(Z), lax.axis_index(X)
    pairs = []
    for a in range(4):
        for b in range(4):
            for k in range(2):
                dz, dx = (a, b) if k == 0 else (b, a)
                block = lax.rem(z + dz, 4) * 4 + lax.rem(x + dx, 4)
                rows = pl.ds(pl.multiple_of(block * 128, 128), 128)
                pairs.append((gathered.at[k, a, b], weight_copy.at[k, rows, :]))
    for src, dst in pairs:
        pltpu.make_async_copy(src, dst, sems.at[0]).start()
    pairs = ((out_1, new_first), (out_2, new_second), (out_w, new_weights), (out_u, update))
    copies = [pltpu.make_async_copy(*pair, sems.at[1 + i]) for i, pair in enumerate(pairs)]
    for copy in copies:
        copy.start()
    for copy in copies:
        copy.wait()
    pltpu.make_async_copy(gathered, gathered, sems.at[0]).wait()


def per_device(*args):
    any_space = pl.BlockSpec(memory_space=pl.ANY)
    vmem_space = pl.BlockSpec(memory_space=pltpu.VMEM)
    held = (
        ((2, 128, 256), F32),
        ((2, 128, 256), F32),
        ((2, 256, 256), F32),
        ((2, 256, 256), F32),
        ((2, 4, 4, 128, 256), BF16),
    )
    dma = pltpu.SemaphoreType.DMA
    results = pl.pallas_call(
        kernel,
        name="step",
        out_shape=[pltpu.VMEM(*shape) for shape in held],
        in_specs=[any_space] * 8,
        out_specs=[vmem_space] * 5,
        scratch_shapes=[
            pltpu.VMEM((2, 4, 2560, 512), BF16),
            pltpu.VMEM((2, 2560, 256), BF16),
            pltpu.VMEM((2, 256, 2560), BF16),
            pltpu.VMEM((2, 4, 512, 256), BF16),
            pltpu.VMEM((2, 4, 4, 256, 128), F32),
            pltpu.VMEM((2, 4, 2, 128, 128), F32),
            pltpu.VMEM((2, 4, 2, 2, 128, 128), F32),
            pltpu.VMEM((2, 2, 128, 128), F32),
            pltpu.VMEM((2, 2, 2, 128, 128), F32),
            pltpu.VMEM((2, 256, 256), F32),
            pltpu.VMEM((2, 2, 32, 256), F32),
            pltpu.VMEM((2, 2, 2, 32, 256), F32),
            pltpu.VMEM((2, 4, 64, 256), F32),
            pltpu.VMEM((2, 256, 256), F32),
            pltpu.VMEM((2, 128, 256), F32),
            pltpu.VMEM((2, 256, 256), F32),
            pltpu.VMEM((2, 256, 256), F32),
            pltpu.VMEM((2, 128, 256), F32),
            pltpu.VMEM((2, 128, 256), F32),
            pltpu.VMEM((2, 128, 256), F32),
            pltpu.VMEM((2, 2, 256, 256), BF16),
            pltpu.VMEM((2, 256, 256), F32),
            pltpu.VMEM((2, 256, 256), F32),
            pltpu.VMEM((8, 128), F32),
            pltpu.VMEM((8, 128), F32),
            pltpu.VMEM((8, 128), F32),
            pltpu.VMEM((64, 128), F32),
            dma((LOADS,)),
            dma((SENDS,)),
            dma((LANDINGS,)),
        ],
        compiler_params=pltpu.CompilerParams(
            collective_id=0, has_side_effects=True, vmem_limit_bytes=60 * 1024 * 1024
        ),
    )(*args)
    return pl.pallas_call(
        write_out,
        name="write_out",
        out_shape=[jax.ShapeDtypeStruct(shape, kind) for shape, kind in held[:4]]
        + [jax.ShapeDtypeStruct((2, 2048, 256), BF16)],
        in_specs=[vmem_space] * 5,
        out_specs=[any_space] * 5,
        scratch_shapes=[dma((5,))],
        compiler_params=pltpu.CompilerParams(vmem_limit_bytes=1024 * 1024),
    )(*results)


def solution(mesh):
    finer = Mesh(mesh.devices.reshape(4, 4, 4, 2), (Z, X, Y, C))
    in_specs = (
        P(FS, None),
        P(FS, None),
        P(FS, TP),
        P(FS, TP),
        P(None, FS, TP),
        P(),
        P(None, None, TP),
        P(None, None, TP),
    )
    out_specs = (
        P(None, FS, TP),
        P(None, FS, TP),
        P(None, None, TP),
        P(None, None, TP),
        P(None, None, TP),
    )
    return jax.shard_map(per_device, mesh=finer, in_specs=in_specs, out_specs=out_specs, check_vma=False)
```
